256 devices in a mesh: sp: 64 (over z, y, core), tp: 4 (over x).
Axes of the slice: x: 4, y: 4, z: 8, core: 2. Of those that a mesh axis runs over, the one named last changes fastest.
Arguments:
- queries: bfloat16 [8192, 1024], P('sp', 'tp'), may hold values from -600 to 600, as said below
- keys: bfloat16 [8192, 256], P('sp', 'tp'), may hold values from -6 to 6
- values: bfloat16 [8192, 256], P('sp', 'tp'), may hold values from -18 to 18
- forget_prefix_log: float32 [8192, 16], P('sp', 'tp'), as said below
- residual: bfloat16 [8192, 2048], P(('sp', 'tp')), may hold values from -6 to 6
- out_weight: bfloat16 [1024, 2048], replicated, may hold values from -0.1875 to 0.1875
- norm_gain: float32 [2048], replicated, may hold values from 0.1 to 1.9
- routes: int32 [8192, 2], P(('sp', 'tp')), may hold values from 0 to 63, all different within a row; in each aligned block of 32 rows (0 to 31, 32 to 63, ...) at most 2 rows name the same one
- route_weight: float32 [8192, 2], P(('sp', 'tp')), may hold values from 0.1 to 1
- w_gate: bfloat16 [64, 2048, 1024], P('sp', None, 'tp'), may hold values from -0.125 to 0.125
- w_up: bfloat16 [64, 2048, 1024], P('sp', None, 'tp'), may hold values from -0.125 to 0.125
- w_down: bfloat16 [64, 1024, 2048], P('sp', 'tp'), may hold values from -0.1875 to 0.1875
Outputs:
- layer_out: bfloat16 [8192, 2048], P(('sp', 'tp'))
The draws below stay inside these ranges and needn't reach their ends.
Inputs may be any that keep to these rules, and one draw needn't show every extreme that they name: `queries`: queries are of order one except for a few positions. `forget_prefix_log`: never rising along positions. `routes`: within the rows of one device (32 positions in order), no expert is named by more than 2 rows, a bound that some block reaches; the experts of one row differ.
All inputs are finite; a program needn't handle non-finite values.
Results may differ from the reference program's by a relative error of at most 0.013.
Values may be sent and summed in bfloat16 or wider, within the bound.
No kernel may reach another device: no remote copies, remote signals or barrier semaphores. Data moves between devices by JAX's collectives and lax.ppermute only.
A program may use at most 64 MiB of HBM per device.

```python
import math
import jax
import jax.numpy as jnp
import numpy as np
from jax import lax

D = 2048
HEADS = 16
KV_HEADS = 4
HEAD_DIM = 64
D_EXPERT = 1024
TOP = 2
TOK_DEV = 128
LENGTH_POSITIONS = 8192
EXPERTS = 64
CAP = 2
N_SP = 64
N_TP = 4


def drawn_pair(key):
    base = jax.random.fold_in(key, 101)
    key_query, key_keys = jax.random.split(base, 2)
    query_raw = jnp.clip(jax.random.normal(key_query, (LENGTH_POSITIONS, HEADS * HEAD_DIM), jnp.float32), -6.0, 6.0)
    keys_raw = jnp.clip(jax.random.normal(key_keys, (LENGTH_POSITIONS, KV_HEADS * HEAD_DIM), jnp.float32), -6.0, 6.0)
    return (query_raw, keys_raw)


def draw_queries(key, part):
    return drawn_pair(key)[0].astype(jnp.bfloat16)


def draw_keys(key, part):
    return drawn_pair(key)[1].astype(jnp.bfloat16)


def draw_forget_prefix_log(key, part):
    base = jax.random.fold_in(key, 202)
    attended_entries_list = jax.random.split(base, 7)
    slow_share = 0.5
    lagging_attention_heads = jax.random.uniform(attended_entries_list[0], (HEADS,)) < slow_share
    slow_total = jax.random.uniform(attended_entries_list[1], (HEADS,), jnp.float32, 0.4, 1.0)
    fast_reach = jnp.exp(jax.random.uniform(attended_entries_list[2], (HEADS,), jnp.float32, math.log(30.0), math.log(100.0)))
    rate = jnp.where(lagging_attention_heads, slow_total / LENGTH_POSITIONS, 1.0 / fast_reach)
    block_factor = jnp.exp(jax.random.uniform(attended_entries_list[3], (LENGTH_POSITIONS // TOK_DEV, HEADS), jnp.float32, math.log(0.5), math.log(2.0)))
    block_factor = jnp.repeat(block_factor, TOK_DEV, axis=0)
    position_factor = jnp.exp(0.5 * jax.random.normal(attended_entries_list[4], (LENGTH_POSITIONS, HEADS), jnp.float32))
    log_forget_factor = -rate[None, :] * block_factor * position_factor
    position_batches = jax.random.randint(attended_entries_list[5], (2,), 0, LENGTH_POSITIONS)
    position_tallies = jax.random.uniform(attended_entries_list[6], (2, HEADS), jnp.float32, 0.22, 0.51)
    log_forget_factor = log_forget_factor.at[position_batches].add(-position_tallies)
    return jnp.cumsum(log_forget_factor, axis=0)


def steps_of(stream_key, dims, cuts, smallest, high):
    factor_of, own = 1.0, jax.random.fold_in(stream_key, 6)
    for dim, blocks in cuts:
        steps = jnp.exp(jax.random.uniform(jax.random.fold_in(own, dim), (blocks,), jnp.float32, smallest / len(cuts), high / len(cuts)))
        factor_of = factor_of * jnp.repeat(steps, dims[dim] // blocks).reshape([-1 if axis == dim else 1 for axis in range(len(dims))])
    return factor_of


def shared_out(key, own, number, rows, count, top, reach, skew):
    order = jax.random.permutation(key, count)
    crowded, common = shares(count, rows * top, reach, skew, True), shares(count, rows * top, reach, skew, False)
    places = jnp.arange(count)

    def named(lengths, rotation):
        used = int((lengths > 0).sum())
        fixed = max(1, used // 4)
        passed = fixed + (places - fixed + rotation * (used - fixed)) % max(1, count - fixed)
        return jnp.zeros((count,), jnp.int32).at[order[jnp.where(places < fixed, places, passed)]].set(jnp.asarray(lengths, jnp.int32))

    lengths = jnp.where(number % 4 == 0, named(crowded, number // 4), named(common, number - number // 4 - 1))
    mixed = jax.random.permutation(jax.random.fold_in(own, 3), count)
    giver, receiver = mixed[0:count // 2 * 2:2], mixed[1:count // 2 * 2:2]
    margin = jnp.minimum(lengths[giver] - 1, reach - lengths[receiver]) // 2
    margin = jnp.where((giver == order[0]) | (receiver == order[0]) | (lengths[receiver] == 0), 0, jnp.maximum(margin, 0))
    passed = jax.random.randint(jax.random.fold_in(own, 4), (count // 2,), 0, 1 << 20) % (margin + 1)
    lengths = lengths.at[giver].add(-passed).at[receiver].add(passed)
    members = jnp.searchsorted(jnp.cumsum(lengths), jnp.arange(rows * top), side="right").astype(jnp.int32)
    grid = members.reshape(top, rows).T
    grid = grid[jax.random.permutation(jax.random.fold_in(own, 1), rows)]
    rotation = jax.random.randint(jax.random.fold_in(own, 2), (rows, 1), 0, top)
    return jnp.take_along_axis(grid, (jnp.arange(top)[None, :] + rotation) % top, axis=1)


def shares(amount, total, bound, skew, full):
    loads = [(1 << 20) // math.isqrt(grade ** skew) + 1 for grade in range(1, amount + 1)]
    largest = bound if full else min(bound, max(-(-total // amount), total * loads[0] // sum(loads)))
    least = 1 if total - largest >= amount - 1 else 0
    given, rest = [largest] + [least] * (amount - 1), total - largest - least * (amount - 1)
    while rest > 0:
        movable = [i for i in range(1, amount) if given[i] < largest] or [i for i in range(1, amount) if given[i] < bound]
        whole, budget = sum([loads[i] for i in movable]), rest
        for i in movable:
            more = min(bound - given[i], max(1, budget * loads[i] // whole), rest)
            given[i] = given[i] + more
            rest = rest - more
    return np.array(given)


def scatter_about(rng, extent, deviation, bound, cuts=(), held_as=jnp.bfloat16):
    array = jax.random.normal(rng, extent, jnp.float32) * deviation
    if len(cuts) > 0:
        array = steps_of(rng, extent, cuts, -0.22, 0.18) * array
    return jnp.clip(array, min=-bound, max=bound).astype(held_as)


def setup_inputs(seed: int = 0) -> dict:
    streams_of = jax.random.split(jax.random.key(seed), 13)
    queries = draw_queries(jax.random.fold_in(streams_of[12], 71), 0)
    keys = draw_keys(jax.random.fold_in(streams_of[12], 71), 0)
    values = scatter_about(streams_of[2], (LENGTH_POSITIONS, KV_HEADS * HEAD_DIM), 3.0, 18.0, ((0, 64), (1, 4)))
    forget_prefix_log = draw_forget_prefix_log(jax.random.fold_in(streams_of[12], 71), 0)
    residual = scatter_about(streams_of[4], (LENGTH_POSITIONS, D), 1.0, 6.0, ((0, 256),))
    out_weight = scatter_about(streams_of[5], (HEADS * HEAD_DIM, D), (HEADS * HEAD_DIM) ** -0.5, 0.1875)
    norm_gain = jnp.clip(1.0 + 0.18 * jax.random.normal(streams_of[6], (D,), jnp.float32), 0.1, 1.9)
    routes_keys = jax.random.split(jax.random.fold_in(streams_of[7], 1), LENGTH_POSITIONS // (TOK_DEV // N_TP))
    routes_turns = jax.random.permutation(jax.random.fold_in(streams_of[7], 3), LENGTH_POSITIONS // (TOK_DEV // N_TP))
    routes = jax.vmap(lambda own, number: shared_out(jax.random.fold_in(streams_of[7], 2), own, number, TOK_DEV // N_TP, EXPERTS, TOP, CAP, 1))(routes_keys, routes_turns).reshape((LENGTH_POSITIONS, TOP))
    route_weight = jnp.clip(0.1 + 0.9 * jax.random.uniform(streams_of[8], (LENGTH_POSITIONS, TOP), jnp.float32) ** steps_of(streams_of[8], (LENGTH_POSITIONS, TOP), ((0, 256),), -0.2, 0.2), 0.1, 1.0)
    w_gate = scatter_about(streams_of[9], (EXPERTS, D, D_EXPERT), D ** -0.5, 0.125, ((0, 64), (2, 4)))
    w_up = scatter_about(streams_of[10], (EXPERTS, D, D_EXPERT), D ** -0.5, 0.125, ((0, 64), (2, 4)))
    w_down = scatter_about(streams_of[11], (EXPERTS, D_EXPERT, D), D_EXPERT ** -0.5, 0.1875, ((0, 64), (1, 4)))
    return dict(queries=queries, keys=keys, values=values, forget_prefix_log=forget_prefix_log, residual=residual, out_weight=out_weight, norm_gain=norm_gain, routes=routes, route_weight=route_weight, w_gate=w_gate, w_up=w_up, w_down=w_down)


def reference(queries, keys, values, forget_prefix_log, residual, out_weight, norm_gain, routes, route_weight, w_gate, w_up, w_down):
    group_size = HEADS // KV_HEADS
    block_rows = math.gcd(LENGTH_POSITIONS, 128)
    score_scale = HEAD_DIM ** (-0.5)
    query_all = queries.astype(jnp.float32).reshape(LENGTH_POSITIONS, KV_HEADS, group_size, HEAD_DIM)
    key_all = keys.astype(jnp.float32).reshape(LENGTH_POSITIONS, KV_HEADS, HEAD_DIM)
    value_all = values.astype(jnp.float32).reshape(LENGTH_POSITIONS, KV_HEADS, HEAD_DIM)
    gates_heads = forget_prefix_log.reshape(LENGTH_POSITIONS, KV_HEADS, group_size).transpose(1, 2, 0)
    key_pos = jnp.arange(LENGTH_POSITIONS, dtype=jnp.int32)

    def attend_block(block_index):
        first_row = (block_index * block_rows).astype(jnp.int32)
        query_block = lax.dynamic_slice_in_dim(query_all, first_row, block_rows, 0)
        gate_block = lax.dynamic_slice_in_dim(gates_heads, first_row, block_rows, 2)
        scores = jnp.einsum('tkgd,skd->kgts', query_block, key_all) * score_scale
        scores = scores + gate_block[..., None] - gates_heads[:, :, None, :]
        causal = (first_row + jnp.arange(block_rows, dtype=jnp.int32))[:, None] >= key_pos[None, :]
        scores = jnp.where(causal, scores, -1e+30)
        row_peak = lax.optimization_barrier(jnp.max(scores, axis=-1, keepdims=True))
        weights = jnp.where(causal, jnp.exp(scores - row_peak), 0.0)
        row_total = lax.optimization_barrier(jnp.sum(weights, axis=-1))
        rounded = lax.optimization_barrier(weights.astype(jnp.bfloat16)).astype(jnp.float32)
        weighted = jnp.einsum('kgts,skd->tkgd', rounded, value_all)
        result = weighted / row_total.transpose(2, 0, 1)[..., None]
        return result.astype(jnp.bfloat16).reshape(block_rows, HEADS * HEAD_DIM)
    attended = lax.map(attend_block, jnp.arange(LENGTH_POSITIONS // block_rows, dtype=jnp.int32))
    attended = attended.reshape(LENGTH_POSITIONS, HEADS * HEAD_DIM)
    stream = residual.astype(jnp.float32) + jnp.dot(attended, out_weight, preferred_element_type=jnp.float32)
    mean_square = lax.optimization_barrier(jnp.mean(stream * stream, axis=-1, keepdims=True))
    normed = (stream * lax.rsqrt(mean_square + 1e-06) * norm_gain.astype(jnp.float32)).astype(jnp.bfloat16)
    assigned = LENGTH_POSITIONS * TOP
    flat_expert = routes.reshape(assigned)
    flat_weight = route_weight.reshape(assigned)
    order = jnp.argsort(flat_expert, stable=True).astype(jnp.int32)
    counts = lax.optimization_barrier(jnp.sum((flat_expert[:, None] == jnp.arange(EXPERTS, dtype=jnp.int32)[None, :]).astype(jnp.int32), axis=0))
    starts = jnp.cumsum(counts) - counts
    most_rows = N_SP * N_TP * CAP
    quarter = D_EXPERT // N_TP

    def one_expert(running_total, expert):
        offsets = jnp.arange(most_rows, dtype=jnp.int32)
        valid = offsets < counts[expert]
        chosen = order[jnp.minimum(starts[expert] + offsets, assigned - 1)]
        position = chosen // TOP
        picked = normed[position]
        gate_act = jnp.dot(picked, w_gate[expert], preferred_element_type=jnp.float32)
        up_act = jnp.dot(picked, w_up[expert], preferred_element_type=jnp.float32)
        activated = (jax.nn.silu(gate_act) * up_act).astype(jnp.bfloat16)
        summed = jnp.zeros((most_rows, D), jnp.float32)
        for quarter_index in range(N_TP):
            partial_out = jnp.dot(activated[:, quarter_index * quarter:(quarter_index + 1) * quarter], w_down[expert][quarter_index * quarter:(quarter_index + 1) * quarter], preferred_element_type=jnp.float32).astype(jnp.bfloat16)
            summed = summed + lax.optimization_barrier(partial_out).astype(jnp.float32)
        expert_out = lax.optimization_barrier(summed.astype(jnp.bfloat16)).astype(jnp.float32)
        scaled = jnp.where(valid, flat_weight[chosen], 0.0)
        return (running_total.at[position].add(scaled[:, None] * expert_out), None)
    mixture, unused = lax.scan(one_expert, jnp.zeros((LENGTH_POSITIONS, D), jnp.float32), jnp.arange(EXPERTS, dtype=jnp.int32))
    return (stream + mixture).astype(jnp.bfloat16)
```

```python
import jax
import jax.numpy as jnp
from jax import lax
from jax.experimental import pallas as pl
from jax.experimental.pallas import tpu as pltpu
from jax.sharding import Mesh, PartitionSpec as P


NZ, NY, NC, NT = 8, 4, 2, 4
TOK = 128
HEAD = 64
HEADS = 4
ROW = 32
D = 2048
BLOCK = TOK + 16
BF16_MAX = 3.3895313892515355e38
NEG = -3.0e38
F32 = jnp.float32
BF16 = jnp.bfloat16
SP = ("z", "y", "c")
PARAMS = pltpu.CompilerParams(vmem_limit_bytes=56 * 1024 * 1024)


def dot(a, b):
    return jnp.dot(a, b, preferred_element_type=F32)


def parts3(x):
    hi = jnp.clip(x, -BF16_MAX, BF16_MAX).astype(BF16)
    rest = x - hi.astype(F32)
    mid = rest.astype(BF16)
    low = (rest - mid.astype(F32)).astype(BF16)
    return hi, mid, low


def pack_kernel(keys_ref, values_ref, gates_ref, out_ref):
    out_ref[0:TOK, :] = jnp.concatenate([keys_ref[...], values_ref[...]], axis=1)
    hi, mid, low = parts3(gates_ref[...])
    rows = [hi.astype(F32), mid.astype(F32), low.astype(F32), jnp.zeros((4, TOK), F32)]
    out_ref[TOK:BLOCK, :] = jnp.concatenate(rows, axis=0).astype(BF16)


def attention_kernel(place_ref, query_ref, *refs):
    chunks, (out_ref, q_scr, m_scr, l_scr, acc_scr) = refs[: NY * NC], refs[NY * NC :]
    own_z, own_order = place_ref[0], place_ref[1]
    for h in range(HEADS):
        part = query_ref[:, h * HEAD : (h + 1) * HEAD] * jnp.asarray(0.125, BF16)
        q_scr[h] = jnp.concatenate([part, jnp.zeros((TOK, HEAD), BF16)], axis=1)

    def loaded(z):
        kv = jnp.concatenate([ref[z, 0:TOK, :] for ref in chunks], axis=0)
        raw = [ref[z, TOK:BLOCK, :].astype(F32) for ref in chunks]
        gates = jnp.concatenate([g[0:4] + g[4:8] + g[8:12] for g in raw], axis=1)
        return kv, gates

    def scores_of(h, kv, gates):
        product = lax.dot_general(
            q_scr[h], kv, (((1,), (1,)), ((), ())), preferred_element_type=F32
        )
        return product - gates[h : h + 1, :]

    def folded(weights):
        total = weights[:, 0:TOK]
        for j in range(1, len(chunks)):
            total = total + weights[:, j * TOK : (j + 1) * TOK]
        return total

    def wide(x):
        return jnp.concatenate([x] * len(chunks), axis=1)

    row = lax.broadcasted_iota(jnp.int32, (TOK, TOK), 0)
    col = lax.broadcasted_iota(jnp.int32, (TOK, TOK), 1)
    limit = []
    for j in range(len(chunks)):
        order = place_ref[2 + j]
        shift = jnp.where(order < own_order, TOK, jnp.where(order == own_order, 0, -TOK))
        limit.append(row + shift - col)
    mask = jnp.concatenate(limit, axis=1) >= 0
    kv, gates = loaded(own_z)
    for h in range(HEADS):
        scores = jnp.where(mask, scores_of(h, kv, gates), NEG)
        peak = jnp.broadcast_to(jnp.max(scores, axis=1, keepdims=True), (TOK, TOK))
        weights = jnp.where(mask, jnp.exp(scores - wide(peak)), 0.0)
        m_scr[h] = peak
        l_scr[h] = folded(weights)
        acc_scr[h] = dot(weights.astype(BF16), kv)

    def body(z, carry):
        kv, gates = loaded(z)
        for h in range(HEADS):
            scores = scores_of(h, kv, gates)
            before = m_scr[h]
            peak = jnp.maximum(before, jnp.max(scores, axis=1, keepdims=True))
            weights = jnp.exp(scores - wide(peak))
            shrink = jnp.exp(before - peak)
            m_scr[h] = peak
            l_scr[h] = l_scr[h] * shrink + folded(weights)
            acc_scr[h] = acc_scr[h] * shrink + dot(weights.astype(BF16), kv)
        return carry

    lax.fori_loop(0, own_z, body, 0)
    done = []
    for h in range(HEADS):
        total = jnp.sum(l_scr[h], axis=1, keepdims=True)
        done.append((acc_scr[h][:, HEAD:] / total).astype(BF16))
    out_ref[...] = jnp.concatenate(done, axis=1)


def attention(place, queries, chunks):
    vmem = pl.BlockSpec(memory_space=pltpu.VMEM)
    return pl.pallas_call(
        attention_kernel,
        out_shape=jax.ShapeDtypeStruct((TOK, HEADS * HEAD), BF16),
        in_specs=[pl.BlockSpec(memory_space=pltpu.SMEM)] + [vmem] * (1 + len(chunks)),
        out_specs=vmem,
        scratch_shapes=[
            pltpu.VMEM((HEADS, TOK, TOK), BF16),
            pltpu.VMEM((HEADS, TOK, TOK), F32),
            pltpu.VMEM((HEADS, TOK, TOK), F32),
            pltpu.VMEM((HEADS, TOK, TOK), F32),
        ],
        compiler_params=PARAMS,
        name="attend",
    )(place, queries, *chunks)


def picks(routes_ref, transposed_slots=128):
    slot = lax.broadcasted_iota(jnp.int32, (transposed_slots, ROW), 0)
    expert, rank = slot // 2, slot % 2
    named0 = routes_ref[0:1, :] == expert
    named1 = routes_ref[1:2, :] == expert
    named = jnp.where(named0 | named1, 1.0, 0.0)
    earlier = lax.broadcasted_iota(jnp.int32, (ROW, ROW), 0) < lax.broadcasted_iota(
        jnp.int32, (ROW, ROW), 1
    )
    before = dot(named.astype(BF16), jnp.where(earlier, 1.0, 0.0).astype(BF16))
    chosen = before == rank.astype(F32)
    return chosen & named0, chosen & named1


def project_kernel(att_ref, weight_ref, residual_ref, gain_ref, routes_ref, stream_ref, rows_ref):
    total = residual_ref[...].astype(F32)
    both = jnp.concatenate([att_ref[x] for x in range(NT)], axis=1)
    total = total + dot(both, weight_ref[...])
    stream_ref[...] = total
    mean_square = jnp.mean(total * total, axis=1, keepdims=True)
    normed = (total * lax.rsqrt(mean_square + 1e-06) * gain_ref[...]).astype(BF16)
    first, second = picks(routes_ref)
    pick = jnp.where(first | second, 1.0, 0.0).astype(BF16)
    rows_ref[...] = dot(pick, normed).astype(BF16)


def hidden_kernel(gate_ref, up_ref, *refs):
    inputs, outs = refs[: len(refs) // 2], refs[len(refs) // 2 :]
    for rows_ref, out_ref in zip(inputs, outs):
        rows = rows_ref[...]
        gate = dot(rows, gate_ref[...])
        up = dot(rows, up_ref[...])
        out_ref[...] = (gate / (1.0 + jnp.exp(-gate)) * up).astype(BF16)


def down_kernel(*refs):
    out_ref = refs[-1]
    half = (len(refs) - 1) // 2
    total = None
    for hidden_ref, weight_ref in zip(refs[:half], refs[half:-1]):
        part = dot(hidden_ref[...], weight_ref[...])
        total = part if total is None else total + part
    out_ref[...] = total.astype(BF16)


def combine_kernel(stream_ref, routes_ref, weight_ref, back_ref, out_ref):
    first, second = picks(routes_ref)
    spread = jnp.where(first, weight_ref[0:1, :], 0.0) + jnp.where(second, weight_ref[1:2, :], 0.0)
    back = back_ref[...]
    total = stream_ref[...]
    for part in parts3(spread):
        total = total + lax.dot_general(
            part, back, (((0,), (0,)), ((), ())), preferred_element_type=F32
        )
    out_ref[...] = total.astype(BF16)


def call(kernel, shapes, *args):
    return pl.pallas_call(
        kernel,
        out_shape=[jax.ShapeDtypeStruct(s, t) for s, t in shapes],
        compiler_params=PARAMS,
        name=kernel.__name__,
    )(*args)


def moved(x, axis, by):
    size = {"z": NZ, "y": NY, "c": NC, "tp": NT}[axis]
    return lax.ppermute(x, axis, [(i, (i + by) % size) for i in range(size)])


def ring(x):
    half = x.shape[0] // 2
    left, right = moved(x, "tp", 1), moved(x, "tp", -1)
    return left, right, moved(left[:half], "tp", 1), moved(right[half:], "tp", -1)


def shards(
    queries,
    keys,
    values,
    forget_prefix_log,
    residual,
    out_weight,
    norm_gain,
    routes,
    route_weight,
    w_gate,
    w_up,
    w_down,
):
    z, y, c = lax.axis_index("z"), lax.axis_index("y"), lax.axis_index("c")
    (block,) = call(pack_kernel, [((BLOCK, TOK), BF16)], keys, values, forget_prefix_log.T)
    down_own = w_down[0]
    down_left, down_right, down_far0, down_far1 = ring(down_own)

    copies = jnp.broadcast_to(block, (NZ, BLOCK, TOK))
    own = lax.all_to_all(copies, "z", 0, 0, tiled=True)
    chunks, orders = [], []
    for step in (0, 1, 3, 2):
        chunk = moved(own, "y", step) if step else own
        from_y = (y - step) % NY
        chunks += [chunk, moved(chunk, "c", 1)]
        orders += [from_y * NC + c, from_y * NC + 1 - c]
    place = jnp.stack([z, y * NC + c] + orders).astype(jnp.int32)
    attended = attention(place, queries, chunks)

    heads = lax.all_to_all(attended.reshape(NT, ROW, -1), "tp", 0, 0, tiled=True)
    routes_row = routes.T
    stream, rows = call(
        project_kernel,
        [((ROW, D), F32), ((TOK, D), BF16)],
        heads,
        out_weight,
        residual,
        norm_gain.reshape(1, D),
        routes_row,
    )
    arrived = lax.all_to_all(rows.reshape(64, 2, D), SP, 0, 0, tiled=True).reshape(TOK, D)
    left, right, far0, far1 = ring(arrived)
    wide = w_gate.shape[2]
    h_own, h_left, h_right, h_far0, h_far1 = call(
        hidden_kernel,
        [((r, wide), BF16) for r in (TOK, TOK, TOK, TOK // 2, TOK // 2)],
        w_gate[0],
        w_up[0],
        arrived,
        left,
        right,
        far0,
        far1,
    )
    from_right = moved(h_left, "tp", -1)
    from_left = moved(h_right, "tp", 1)
    from_far = moved(jnp.concatenate([h_far0, h_far1]), "tp", 2)
    half = wide // 2
    (expert_out,) = call(
        down_kernel,
        [((TOK, D), BF16)],
        h_own,
        from_left,
        from_right,
        from_far[:, :half],
        from_far[:, half:],
        down_own,
        down_left,
        down_right,
        down_far0,
        down_far1,
    )
    back = lax.all_to_all(expert_out.reshape(64, 2, D), SP, 0, 0, tiled=True).reshape(TOK, D)
    (out,) = call(
        combine_kernel, [((ROW, D), BF16)], stream, routes_row, route_weight.T, back
    )
    return out


def solution(mesh):
    split = Mesh(mesh.devices.reshape(NZ, NY, NC, NT), ("z", "y", "c", "tp"))
    rows = P(("z", "y", "c", "tp"), None)
    return jax.shard_map(
        shards,
        mesh=split,
        in_specs=(
            P(SP, "tp"),
            P(SP, "tp"),
            P(SP, "tp"),
            P(SP, "tp"),
            rows,
            P(),
            P(),
            rows,
            rows,
            P(SP, None, "tp"),
            P(SP, None, "tp"),
            P(SP, "tp", None),
        ),
        out_specs=rows,
        check_vma=False,
    )
```

```python
import functools

import jax
import jax.numpy as jnp
from jax import lax
from jax.experimental import pallas as pl
from jax.experimental.pallas import tpu as pltpu
from jax.sharding import Mesh, PartitionSpec as P


NZ, NY, NC, NT = 8, 4, 2, 4
TOK = 128
HEAD = 64
HEADS = 4
ROW = 32
D = 2048
BLOCK = TOK + 16
GROUP = 2
BF16_MAX = 3.3895313892515355e38
NEG = -3.0e38
F32 = jnp.float32
BF16 = jnp.bfloat16
SP = ("z", "y", "c")
PARAMS = pltpu.CompilerParams(vmem_limit_bytes=24 * 1024 * 1024)


def in_hbm(x):
    return pltpu.with_memory_space_constraint(x, pltpu.HBM)


def in_vmem(x):
    return pltpu.with_memory_space_constraint(x, pltpu.VMEM)


def dot(a, b):
    return jnp.dot(a, b, preferred_element_type=F32)


def parts3(x):
    hi = jnp.clip(x, -BF16_MAX, BF16_MAX).astype(BF16)
    rest = x - hi.astype(F32)
    mid = rest.astype(BF16)
    low = (rest - mid.astype(F32)).astype(BF16)
    return hi, mid, low


def fetches(pairs, sems):
    return [pltpu.make_async_copy(src, dst, sems.at[i]) for i, (src, dst) in enumerate(pairs)]


def pack_kernel(keys_hbm, values_hbm, gates_hbm, out_ref, keys_ref, values_ref, gates_ref, sems):
    copies = fetches(
        [(gates_hbm, gates_ref), (keys_hbm, keys_ref), (values_hbm, values_ref)], sems
    )
    for copy in copies:
        copy.start()
    for copy in copies:
        copy.wait()
    hi, mid, low = parts3(gates_ref[...])
    rows = [hi.astype(F32), mid.astype(F32), low.astype(F32), jnp.zeros((4, TOK), F32)]
    gates = jnp.concatenate(rows, axis=0).astype(BF16)
    for z in range(NZ):
        out_ref[z, 0:HEAD, :] = keys_ref[...]
        out_ref[z, HEAD : HEAD + 16, :] = gates
        out_ref[z, HEAD + 16 : BLOCK, :] = values_ref[...]


def pack(keys, values, gates):
    hbm = pl.BlockSpec(memory_space=pltpu.HBM)
    return pl.pallas_call(
        pack_kernel,
        out_shape=jax.ShapeDtypeStruct((NZ, BLOCK, TOK), BF16),
        in_specs=[hbm] * 3,
        out_specs=pl.BlockSpec(memory_space=pltpu.VMEM),
        scratch_shapes=[
            pltpu.VMEM((HEAD, TOK), BF16),
            pltpu.VMEM((HEAD, TOK), BF16),
            pltpu.VMEM((HEADS, TOK), F32),
            pltpu.SemaphoreType.DMA((3,)),
        ],
        compiler_params=PARAMS,
        name="pack",
    )(in_hbm(keys), in_hbm(values), in_hbm(gates))


def query_rows(query_ref):
    col = lax.broadcasted_iota(jnp.int32, (TOK, 16), 1)
    rows = []
    for h in range(HEADS):
        part = query_ref[:, h * HEAD : (h + 1) * HEAD] * jnp.asarray(0.125, BF16)
        takes = (col % HEADS == h) & (col < 3 * HEADS) | (col == 3 * HEADS)
        rows.append(jnp.concatenate([part, jnp.where(takes, -1.0, 0.0).astype(BF16)], axis=1))
    return jnp.concatenate(rows, axis=0)


def attend_kernel(count, place_ref, query_hbm, source_ref, *refs):
    chunks, refs = refs[:count], refs[count:]
    out_ref, target_ref, m_ref, l_ref, acc_ref, query_ref, sems = refs
    fetch, copy = fetches([(query_hbm, query_ref), (source_ref, target_ref)], sems)
    fetch.start()
    copy.start()
    fetch.wait()
    own_z, own_order = place_ref[0], place_ref[1]
    queries = query_rows(query_ref)
    total_rows = HEADS * TOK
    blocks = GROUP * count
    row_of_gate = lax.broadcasted_iota(jnp.int32, (16, TOK), 0)

    def folded(weights):
        total = weights[:, 0:TOK]
        for j in range(1, blocks):
            total = total + weights[:, j * TOK : (j + 1) * TOK]
        return total

    def step(base, first):
        key_rows, value_rows, shifts = [], [], []
        for g in range(GROUP):
            for j, ref in enumerate(chunks):
                gates = ref[base + g, HEAD : HEAD + 16, :]
                if first:
                    order = place_ref[2 + j]
                    seen = (base + g < own_z) | ((base + g == own_z) & (order <= own_order))
                    bar = jnp.where(seen, 0.0, -NEG).astype(BF16)
                    gates = jnp.where(row_of_gate == 3 * HEADS, bar, gates)
                    shifts.append(jnp.where((base + g == own_z) & (order == own_order), 0, TOK))
                key_rows.append(jnp.concatenate([ref[base + g, 0:HEAD, :], gates], axis=0))
                value_rows.append(ref[base + g, HEAD + 16 : BLOCK, :])
        scores = dot(queries, jnp.concatenate(key_rows, axis=1))
        if first:
            ahead = lax.broadcasted_iota(jnp.int32, (total_rows, TOK), 0) % TOK
            ahead = ahead - lax.broadcasted_iota(jnp.int32, (total_rows, TOK), 1)
            pieces = []
            for i in range(blocks):
                piece = scores[:, i * TOK : (i + 1) * TOK]
                if i % count == 0:
                    piece = jnp.where(ahead + shifts[i] >= 0, piece, NEG)
                pieces.append(piece)
            scores = jnp.concatenate(pieces, axis=1)
        peak = jnp.max(scores, axis=1, keepdims=True)
        if first:
            peak = jnp.broadcast_to(peak, (total_rows, TOK))
        else:
            before = m_ref[...]
            peak = jnp.maximum(before, peak)
        weights = jnp.exp(scores - jnp.concatenate([peak] * blocks, axis=1))
        product = lax.dot_general(
            weights.astype(BF16),
            jnp.concatenate(value_rows, axis=1),
            (((1,), (1,)), ((), ())),
            preferred_element_type=F32,
        )
        m_ref[...] = peak
        if first:
            l_ref[...] = folded(weights)
            acc_ref[...] = product
        else:
            shrink = jnp.exp(before - peak)
            l_ref[...] = l_ref[...] * shrink + folded(weights)
            acc_ref[...] = acc_ref[...] * shrink[:, :HEAD] + product

    groups = own_z // GROUP
    step(groups * GROUP, True)

    def body(group, carry):
        step(group * GROUP, False)
        return carry

    lax.fori_loop(0, groups, body, 0)
    done = []
    for h in range(HEADS):
        here = slice(h * TOK, (h + 1) * TOK)
        total = jnp.sum(l_ref[here, :], axis=1, keepdims=True)
        done.append((acc_ref[here, :] / total).astype(BF16))
    out_ref[...] = jnp.concatenate(done, axis=1)
    copy.wait()


def attend(place, queries, weight, chunks):
    vmem = pl.BlockSpec(memory_space=pltpu.VMEM)
    total_rows = HEADS * TOK
    return pl.pallas_call(
        functools.partial(attend_kernel, len(chunks)),
        out_shape=[
            jax.ShapeDtypeStruct((TOK, HEADS * HEAD), BF16),
            jax.ShapeDtypeStruct(weight.shape, weight.dtype),
        ],
        in_specs=[pl.BlockSpec(memory_space=pltpu.SMEM)]
        + [pl.BlockSpec(memory_space=pltpu.HBM)] * 2
        + [vmem] * len(chunks),
        out_specs=[vmem] * 2,
        scratch_shapes=[
            pltpu.VMEM((total_rows, TOK), F32),
            pltpu.VMEM((total_rows, TOK), F32),
            pltpu.VMEM((total_rows, HEAD), F32),
            pltpu.VMEM(queries.shape, BF16),
            pltpu.SemaphoreType.DMA((2,)),
        ],
        compiler_params=PARAMS,
        name="attend",
    )(place, in_hbm(queries), in_hbm(weight), *map(in_vmem, chunks))


def picks(routes_ref, transposed_slots=128):
    slot = lax.broadcasted_iota(jnp.int32, (transposed_slots, ROW), 0)
    expert, rank = slot // 2, slot % 2
    named0 = routes_ref[0:1, :] == expert
    named1 = routes_ref[1:2, :] == expert
    named = jnp.where(named0 | named1, 1.0, 0.0)
    earlier = lax.broadcasted_iota(jnp.int32, (ROW, ROW), 0) < lax.broadcasted_iota(
        jnp.int32, (ROW, ROW), 1
    )
    before = dot(named.astype(BF16), jnp.where(earlier, 1.0, 0.0).astype(BF16))
    chosen = before == rank.astype(F32)
    return chosen & named0, chosen & named1


def project_kernel(att_ref, weight_ref, residual_ref, gain_ref, routes_ref, stream_ref, rows_ref):
    total = residual_ref[...].astype(F32)
    both = jnp.concatenate([att_ref[x] for x in range(NT)], axis=1)
    total = total + dot(both, weight_ref[...])
    stream_ref[...] = total
    mean_square = jnp.mean(total * total, axis=1, keepdims=True)
    normed = (total * lax.rsqrt(mean_square + 1e-06) * gain_ref[...]).astype(BF16)
    first, second = picks(routes_ref)
    pick = jnp.where(first | second, 1.0, 0.0).astype(BF16)
    rows_ref[...] = dot(pick, normed).astype(BF16)


def hidden(rows, gate_ref, up_ref):
    gate = dot(rows, gate_ref[...])
    up = dot(rows, up_ref[...])
    return (gate / (1.0 + jnp.exp(-gate)) * up).astype(BF16)


def near_kernel(own_ref, left_ref, right_ref, *refs):
    sources, (h_own, h_left, h_right), refs = refs[:6], refs[6:9], refs[9:]
    targets, sems = refs[:6], refs[6]
    copies = fetches(list(zip(sources, targets)), sems)
    for copy in copies:
        copy.start()
    copies[0].wait()
    copies[1].wait()
    for rows_ref, out_ref in ((own_ref, h_own), (left_ref, h_left), (right_ref, h_right)):
        out_ref[...] = hidden(rows_ref[...], targets[0], targets[1])
    for copy in copies[2:]:
        copy.wait()


def near(rows, weights):
    vmem = pl.BlockSpec(memory_space=pltpu.VMEM)
    shape = jax.ShapeDtypeStruct((TOK, weights[0].shape[1]), BF16)
    return pl.pallas_call(
        near_kernel,
        out_shape=[shape] * 3 + [jax.ShapeDtypeStruct(w.shape, w.dtype) for w in weights],
        in_specs=[vmem] * 3 + [pl.BlockSpec(memory_space=pltpu.HBM)] * 6,
        out_specs=[vmem] * 9,
        scratch_shapes=[pltpu.SemaphoreType.DMA((6,))],
        compiler_params=PARAMS,
        name="near",
    )(*rows, *map(in_hbm, weights))


def far_kernel(gate_ref, up_ref, far0_ref, far1_ref, out_ref):
    half = TOK // 2
    out_ref[:half, :] = hidden(far0_ref[...], gate_ref, up_ref)
    out_ref[half:, :] = hidden(far1_ref[...], gate_ref, up_ref)


def down_kernel(own_ref, left_ref, right_ref, far_ref, w_own, w_left, w_right, w_far, out_ref):
    total = dot(own_ref[...], w_own[...])
    total = total + dot(left_ref[...], w_left[...])
    total = total + dot(right_ref[...], w_right[...])
    out_ref[...] = (total + dot(far_ref[...], w_far[...])).astype(BF16)


def combine_kernel(stream_ref, routes_ref, weight_ref, back_ref, out_ref):
    first, second = picks(routes_ref)
    spread = jnp.where(first, weight_ref[0:1, :], 0.0) + jnp.where(second, weight_ref[1:2, :], 0.0)
    back = back_ref[...]
    total = stream_ref[...]
    for part in parts3(spread):
        total = total + lax.dot_general(
            part, back, (((0,), (0,)), ((), ())), preferred_element_type=F32
        )
    out_ref[...] = total.astype(BF16)


def call(kernel, shapes, *args):
    return pl.pallas_call(
        kernel, out_shape=[jax.ShapeDtypeStruct(s, t) for s, t in shapes], compiler_params=PARAMS
    )(*args)


def moved(x, axis, by):
    size = {"z": NZ, "y": NY, "c": NC, "tp": NT}[axis]
    return lax.ppermute(x, axis, [(i, (i + by) % size) for i in range(size)])


def shards(
    queries,
    keys,
    values,
    forget_prefix_log,
    residual,
    out_weight,
    norm_gain,
    routes,
    route_weight,
    w_gate,
    w_up,
    w_down,
):
    z, y, c = lax.axis_index("z"), lax.axis_index("y"), lax.axis_index("c")
    down_own = w_down[0]
    down_left, down_right = moved(down_own, "tp", 1), moved(down_own, "tp", -1)
    copies = pack(keys.T, values.T, forget_prefix_log.T)
    own = lax.all_to_all(copies, "z", 0, 0, tiled=True)
    chunks = [own, moved(own, "c", 1)]
    place = [z, y * NC + c, y * NC + c, y * NC + 1 - c]
    for step in (1, 3, 2):
        chunk = moved(own, "y", step)
        from_y = (y - step) % NY
        chunks += [chunk, moved(chunk, "c", 1)]
        place += [from_y * NC + c, from_y * NC + 1 - c]
    place = jnp.stack(place).astype(jnp.int32)
    attended, out_w = attend(place, queries, out_weight, chunks)

    heads = lax.all_to_all(attended.reshape(NT, ROW, -1), "tp", 0, 0, tiled=True)
    far_source, _ = lax.optimization_barrier((down_own, heads))
    down_far = moved(far_source, "tp", 2)
    routes_row = routes.T
    stream, rows = call(
        project_kernel,
        [((ROW, D), F32), ((TOK, D), BF16)],
        heads,
        out_w,
        residual,
        norm_gain.reshape(1, D),
        routes_row,
    )
    arrived = lax.all_to_all(rows.reshape(64, 2, D), SP, 0, 0, tiled=True).reshape(TOK, D)
    left, right = moved(arrived, "tp", 1), moved(arrived, "tp", -1)
    half = TOK // 2
    far0, far1 = moved(left[:half], "tp", 1), moved(right[half:], "tp", -1)
    h_own, h_left, h_right, gate_w, up_w, *down_w = near(
        (arrived, left, right),
        (w_gate[0], w_up[0], down_own, down_left, down_right, down_far),
    )
    (h_far,) = call(far_kernel, [(h_own.shape, BF16)], gate_w, up_w, far0, far1)
    (expert_out,) = call(
        down_kernel,
        [((TOK, D), BF16)],
        h_own,
        moved(h_right, "tp", 1),
        moved(h_left, "tp", -1),
        moved(h_far, "tp", 2),
        *down_w,
    )
    back = lax.all_to_all(expert_out.reshape(64, 2, D), SP, 0, 0, tiled=True).reshape(TOK, D)
    (out,) = call(
        combine_kernel, [((ROW, D), BF16)], stream, routes_row, route_weight.T, back
    )
    return out


def solution(mesh):
    split = Mesh(mesh.devices.reshape(NZ, NY, NC, NT), ("z", "y", "c", "tp"))
    rows = P(("z", "y", "c", "tp"), None)

    return jax.shard_map(
        shards,
        mesh=split,
        in_specs=(
            P(SP, "tp"),
            P(SP, "tp"),
            P(SP, "tp"),
            P(SP, "tp"),
            rows,
            P(),
            P(),
            rows,
            rows,
            P(SP, None, "tp"),
            P(SP, None, "tp"),
            P(SP, "tp", None),
        ),
        out_specs=rows,
        check_vma=False,
    )
```

```python
import functools

import jax
import jax.numpy as jnp
from jax import lax
from jax.experimental import pallas as pl
from jax.experimental.pallas import tpu as pltpu
from jax.sharding import Mesh, PartitionSpec as P


NZ, NY, NC, NT = 8, 4, 2, 4
TOK = 128
HEAD = 64
HEADS = 4
ROW = 32
D = 2048
BLOCK = TOK + 16
GROUP = 2
BF16_MAX = 3.3895313892515355e38
NEG = -3.0e38
F32 = jnp.float32
BF16 = jnp.bfloat16
SP = ("z", "y", "c")
PARAMS = pltpu.CompilerParams(vmem_limit_bytes=24 * 1024 * 1024)


def in_hbm(x):
    return pltpu.with_memory_space_constraint(x, pltpu.HBM)


def in_vmem(x):
    return pltpu.with_memory_space_constraint(x, pltpu.VMEM)


def dot(a, b):
    return jnp.dot(a, b, preferred_element_type=F32)


def parts3(x):
    hi = jnp.clip(x, -BF16_MAX, BF16_MAX).astype(BF16)
    rest = x - hi.astype(F32)
    mid = rest.astype(BF16)
    low = (rest - mid.astype(F32)).astype(BF16)
    return hi, mid, low


def fetches(pairs, sems):
    return [pltpu.make_async_copy(src, dst, sems.at[i]) for i, (src, dst) in enumerate(pairs)]


def pack_kernel(keys_hbm, values_hbm, gates_hbm, out_ref, keys_ref, values_ref, gates_ref, sems):
    copies = fetches(
        [(gates_hbm, gates_ref), (keys_hbm, keys_ref), (values_hbm, values_ref)], sems
    )
    for copy in copies:
        copy.start()
    for copy in copies:
        copy.wait()
    hi, mid, low = parts3(gates_ref[...])
    rows = [hi.astype(F32), mid.astype(F32), low.astype(F32), jnp.zeros((4, TOK), F32)]
    gates = jnp.concatenate(rows, axis=0).astype(BF16)
    for z in range(NZ):
        out_ref[z, 0:HEAD, :] = keys_ref[...]
        out_ref[z, HEAD : HEAD + 16, :] = gates
        out_ref[z, HEAD + 16 : BLOCK, :] = values_ref[...]


def pack(keys, values, gates):
    hbm = pl.BlockSpec(memory_space=pltpu.HBM)
    return pl.pallas_call(
        pack_kernel,
        out_shape=jax.ShapeDtypeStruct((NZ, BLOCK, TOK), BF16),
        in_specs=[hbm] * 3,
        out_specs=pl.BlockSpec(memory_space=pltpu.VMEM),
        scratch_shapes=[
            pltpu.VMEM((HEAD, TOK), BF16),
            pltpu.VMEM((HEAD, TOK), BF16),
            pltpu.VMEM((HEADS, TOK), F32),
            pltpu.SemaphoreType.DMA((3,)),
        ],
        compiler_params=PARAMS,
        name="pack",
    )(in_hbm(keys), in_hbm(values), in_hbm(gates))


def query_rows(query_ref):
    col = lax.broadcasted_iota(jnp.int32, (TOK, 16), 1)
    rows = []
    for h in range(HEADS):
        part = query_ref[:, h * HEAD : (h + 1) * HEAD] * jnp.asarray(0.125, BF16)
        takes = (col % HEADS == h) & (col < 3 * HEADS) | (col == 3 * HEADS)
        rows.append(jnp.concatenate([part, jnp.where(takes, -1.0, 0.0).astype(BF16)], axis=1))
    return jnp.concatenate(rows, axis=0)


def query_kernel(query_ref, out_ref):
    out_ref[...] = query_rows(query_ref)


def attend_kernel(count, place_ref, query_ref, source_ref, *refs):
    chunks, refs = refs[:count], refs[count:]
    out_ref, target_ref, m_ref, l_ref, acc_ref, sem = refs
    copy = pltpu.make_async_copy(source_ref, target_ref, sem)
    copy.start()
    own_z, own_order = place_ref[0], place_ref[1]
    queries = query_ref[...]
    total_rows = HEADS * TOK
    blocks = GROUP * count
    row_of_gate = lax.broadcasted_iota(jnp.int32, (16, TOK), 0)

    def folded(weights):
        total = weights[:, 0:TOK]
        for j in range(1, blocks):
            total = total + weights[:, j * TOK : (j + 1) * TOK]
        return total

    def step(base, first):
        key_rows, value_rows, shifts = [], [], []
        for g in range(GROUP):
            for j, ref in enumerate(chunks):
                gates = ref[base + g, HEAD : HEAD + 16, :]
                if first:
                    order = place_ref[2 + j]
                    seen = (base + g < own_z) | ((base + g == own_z) & (order <= own_order))
                    bar = jnp.where(seen, 0.0, -NEG).astype(BF16)
                    gates = jnp.where(row_of_gate == 3 * HEADS, bar, gates)
                    shifts.append(jnp.where((base + g == own_z) & (order == own_order), 0, TOK))
                key_rows.append(jnp.concatenate([ref[base + g, 0:HEAD, :], gates], axis=0))
                value_rows.append(ref[base + g, HEAD + 16 : BLOCK, :])
        scores = dot(queries, jnp.concatenate(key_rows, axis=1))
        if first:
            ahead = lax.broadcasted_iota(jnp.int32, (total_rows, TOK), 0) % TOK
            ahead = ahead - lax.broadcasted_iota(jnp.int32, (total_rows, TOK), 1)
            pieces = []
            for i in range(blocks):
                piece = scores[:, i * TOK : (i + 1) * TOK]
                if i % count == 0:
                    piece = jnp.where(ahead + shifts[i] >= 0, piece, NEG)
                pieces.append(piece)
            scores = jnp.concatenate(pieces, axis=1)
        peak = jnp.max(scores, axis=1, keepdims=True)
        if first:
            peak = jnp.broadcast_to(peak, (total_rows, TOK))
        else:
            before = m_ref[...]
            peak = jnp.maximum(before, peak)
        weights = jnp.exp(scores - jnp.concatenate([peak] * blocks, axis=1))
        product = lax.dot_general(
            weights.astype(BF16),
            jnp.concatenate(value_rows, axis=1),
            (((1,), (1,)), ((), ())),
            preferred_element_type=F32,
        )
        m_ref[...] = peak
        if first:
            l_ref[...] = folded(weights)
            acc_ref[...] = product
        else:
            shrink = jnp.exp(before - peak)
            l_ref[...] = l_ref[...] * shrink + folded(weights)
            acc_ref[...] = acc_ref[...] * shrink[:, :HEAD] + product

    groups = own_z // GROUP
    step(groups * GROUP, True)

    def body(group, carry):
        step(group * GROUP, False)
        return carry

    lax.fori_loop(0, groups, body, 0)
    done = []
    for h in range(HEADS):
        here = slice(h * TOK, (h + 1) * TOK)
        total = jnp.sum(l_ref[here, :], axis=1, keepdims=True)
        done.append((acc_ref[here, :] / total).astype(BF16))
    out_ref[...] = jnp.concatenate(done, axis=1)
    copy.wait()


def attend(place, queries, weight, chunks):
    vmem = pl.BlockSpec(memory_space=pltpu.VMEM)
    total_rows = HEADS * TOK
    return pl.pallas_call(
        functools.partial(attend_kernel, len(chunks)),
        out_shape=[
            jax.ShapeDtypeStruct((TOK, HEADS * HEAD), BF16),
            jax.ShapeDtypeStruct(weight.shape, weight.dtype),
        ],
        in_specs=[pl.BlockSpec(memory_space=pltpu.SMEM), vmem]
        + [pl.BlockSpec(memory_space=pltpu.HBM)]
        + [vmem] * len(chunks),
        out_specs=[vmem] * 2,
        scratch_shapes=[
            pltpu.VMEM((total_rows, TOK), F32),
            pltpu.VMEM((total_rows, TOK), F32),
            pltpu.VMEM((total_rows, HEAD), F32),
            pltpu.SemaphoreType.DMA,
        ],
        compiler_params=PARAMS,
        name="attend",
    )(place, in_vmem(queries), in_hbm(weight), *map(in_vmem, chunks))


def picks(routes_ref, transposed_slots=128):
    slot = lax.broadcasted_iota(jnp.int32, (transposed_slots, ROW), 0)
    expert, rank = slot // 2, slot % 2
    named0 = routes_ref[0:1, :] == expert
    named1 = routes_ref[1:2, :] == expert
    named = jnp.where(named0 | named1, 1.0, 0.0)
    earlier = lax.broadcasted_iota(jnp.int32, (ROW, ROW), 0) < lax.broadcasted_iota(
        jnp.int32, (ROW, ROW), 1
    )
    before = dot(named.astype(BF16), jnp.where(earlier, 1.0, 0.0).astype(BF16))
    chosen = before == rank.astype(F32)
    return chosen & named0, chosen & named1


def project_kernel(att_ref, weight_ref, residual_ref, gain_ref, routes_ref, stream_ref, rows_ref):
    total = residual_ref[...].astype(F32)
    both = jnp.concatenate([att_ref[x] for x in range(NT)], axis=1)
    total = total + dot(both, weight_ref[...])
    stream_ref[...] = total
    mean_square = jnp.mean(total * total, axis=1, keepdims=True)
    normed = (total * lax.rsqrt(mean_square + 1e-06) * gain_ref[...]).astype(BF16)
    first, second = picks(routes_ref)
    pick = jnp.where(first | second, 1.0, 0.0).astype(BF16)
    rows_ref[...] = dot(pick, normed).astype(BF16)


def hidden(rows, gate_ref, up_ref):
    gate = dot(rows, gate_ref[...])
    up = dot(rows, up_ref[...])
    return (gate / (1.0 + jnp.exp(-gate)) * up).astype(BF16)


def near_kernel(own, left0, right1, *refs):
    sources, outs, targets, sems = refs[:6], refs[6:9], refs[9:15], refs[15]
    copies = fetches(list(zip(sources, targets)), sems)
    for copy in copies:
        copy.start()
    copies[0].wait()
    copies[1].wait()
    for rows, out_ref in zip((own, left0, right1), outs):
        out_ref[...] = hidden(rows[...], targets[0], targets[1])
    for copy in copies[2:]:
        copy.wait()


def near(rows, weights):
    vmem = pl.BlockSpec(memory_space=pltpu.VMEM)
    wide = weights[0].shape[1]
    return pl.pallas_call(
        near_kernel,
        out_shape=[jax.ShapeDtypeStruct((r.shape[0], wide), BF16) for r in rows]
        + [jax.ShapeDtypeStruct(w.shape, w.dtype) for w in weights],
        in_specs=[vmem] * len(rows) + [pl.BlockSpec(memory_space=pltpu.HBM)] * len(weights),
        out_specs=[vmem] * (len(rows) + len(weights)),
        scratch_shapes=[pltpu.SemaphoreType.DMA((len(weights),))],
        compiler_params=PARAMS,
        name="near",
    )(*rows, *map(in_hbm, weights))


def rest_kernel(gate_ref, up_ref, left1, right0, h_left0, h_right1, h_left, h_right):
    half = TOK // 2
    h_left[:half, :] = h_left0[...]
    h_left[half:, :] = hidden(left1[...], gate_ref, up_ref)
    h_right[:half, :] = hidden(right0[...], gate_ref, up_ref)
    h_right[half:, :] = h_right1[...]


def far_kernel(gate_ref, up_ref, far0, far1, h_far):
    rows = jnp.concatenate([far0[...], far1[...]], axis=0)
    h_far[...] = hidden(rows, gate_ref, up_ref)


def down_kernel(own_ref, left_ref, right_ref, far_ref, w_own, w_left, w_right, w_far, out_ref):
    total = dot(own_ref[...], w_own[...])
    total = total + dot(left_ref[...], w_left[...])
    total = total + dot(right_ref[...], w_right[...])
    out_ref[...] = (total + dot(far_ref[...], w_far[...])).astype(BF16)


def combine_kernel(stream_ref, routes_ref, weight_ref, back_ref, out_ref):
    first, second = picks(routes_ref)
    spread = jnp.where(first, weight_ref[0:1, :], 0.0) + jnp.where(second, weight_ref[1:2, :], 0.0)
    back = back_ref[...]
    total = stream_ref[...]
    for part in parts3(spread):
        total = total + lax.dot_general(
            part, back, (((0,), (0,)), ((), ())), preferred_element_type=F32
        )
    out_ref[...] = total.astype(BF16)


def call(kernel, shapes, *args):
    return pl.pallas_call(
        kernel, out_shape=[jax.ShapeDtypeStruct(s, t) for s, t in shapes], compiler_params=PARAMS
    )(*args)


def moved(x, axis, by):
    size = {"z": NZ, "y": NY, "c": NC, "tp": NT}[axis]
    return lax.ppermute(x, axis, [(i, (i + by) % size) for i in range(size)])


def shards(
    queries,
    keys,
    values,
    forget_prefix_log,
    residual,
    out_weight,
    norm_gain,
    routes,
    route_weight,
    w_gate,
    w_up,
    w_down,
):
    z, y, c = lax.axis_index("z"), lax.axis_index("y"), lax.axis_index("c")
    down_own = w_down[0]
    down_left, down_right = moved(down_own, "tp", 1), moved(down_own, "tp", -1)
    copies = pack(keys.T, values.T, forget_prefix_log.T)
    own = lax.all_to_all(copies, "z", 0, 0, tiled=True)
    (rows_of_q,) = call(query_kernel, [((HEADS * TOK, HEAD + 16), BF16)], queries)
    chunks = [own, moved(own, "c", 1)]
    place = [z, y * NC + c, y * NC + c, y * NC + 1 - c]
    for step in (1, 3, 2):
        chunk = moved(own, "y", step)
        from_y = (y - step) % NY
        chunks += [chunk, moved(chunk, "c", 1)]
        place += [from_y * NC + c, from_y * NC + 1 - c]
    place = jnp.stack(place).astype(jnp.int32)
    attended, out_w = attend(place, rows_of_q, out_weight, chunks)

    heads = lax.all_to_all(attended.reshape(NT, ROW, -1), "tp", 0, 0, tiled=True)
    far_source, _ = lax.optimization_barrier((down_own, heads))
    down_far = moved(far_source, "tp", 2)
    routes_row = routes.T
    stream, rows = call(
        project_kernel,
        [((ROW, D), F32), ((TOK, D), BF16)],
        heads,
        out_w,
        residual,
        norm_gain.reshape(1, D),
        routes_row,
    )
    arrived = lax.all_to_all(rows.reshape(64, 2, D), SP, 0, 0, tiled=True).reshape(TOK, D)
    half = TOK // 2
    top, bottom = arrived[:half], arrived[half:]
    left0, right1 = moved(top, "tp", 1), moved(bottom, "tp", -1)
    left1, right0 = moved(bottom, "tp", 1), moved(top, "tp", -1)
    far0, far1 = moved(left0, "tp", 1), moved(right1, "tp", -1)
    h_own, h_left0, h_right1, gate_w, up_w, *down_w = near(
        (arrived, left0, right1),
        (w_gate[0], w_up[0], down_own, down_left, down_right, down_far),
    )
    shape = (h_own.shape, BF16)
    h_left, h_right = call(rest_kernel, [shape] * 2, gate_w, up_w, left1, right0, h_left0, h_right1)
    from_left, from_right = moved(h_right, "tp", 1), moved(h_left, "tp", -1)
    (h_far,) = call(far_kernel, [shape], gate_w, up_w, far0, far1)
    (expert_out,) = call(
        down_kernel,
        [((TOK, D), BF16)],
        h_own,
        from_left,
        from_right,
        moved(h_far, "tp", 2),
        *down_w,
    )
    back = lax.all_to_all(expert_out.reshape(64, 2, D), SP, 0, 0, tiled=True).reshape(TOK, D)
    (out,) = call(
        combine_kernel, [((ROW, D), BF16)], stream, routes_row, route_weight.T, back
    )
    return out


def solution(mesh):
    split = Mesh(mesh.devices.reshape(NZ, NY, NC, NT), ("z", "y", "c", "tp"))
    rows = P(("z", "y", "c", "tp"), None)

    return jax.shard_map(
        shards,
        mesh=split,
        in_specs=(
            P(SP, "tp"),
            P(SP, "tp"),
            P(SP, "tp"),
            P(SP, "tp"),
            rows,
            P(),
            P(),
            rows,
            rows,
            P(SP, None, "tp"),
            P(SP, None, "tp"),
            P(SP, "tp", None),
        ),
        out_specs=rows,
        check_vma=False,
    )
```

```python
import functools

import jax
import jax.numpy as jnp
from jax import lax
from jax.experimental import pallas as pl
from jax.experimental.pallas import tpu as pltpu
from jax.sharding import Mesh, PartitionSpec as P


NZ, NY, NC, NT = 8, 4, 2, 4
TOK = 128
HEAD = 64
HEADS = 4
ROW = 32
D = 2048
BLOCK = TOK + 16
BF16_MAX = 3.3895313892515355e38
NEG = -3.0e38
F32 = jnp.float32
BF16 = jnp.bfloat16
SP = ("z", "y", "c")
PARAMS = pltpu.CompilerParams(vmem_limit_bytes=24 * 1024 * 1024)


def in_hbm(x):
    return pltpu.with_memory_space_constraint(x, pltpu.HBM)


def in_vmem(x):
    return pltpu.with_memory_space_constraint(x, pltpu.VMEM)


def dot(a, b):
    return jnp.dot(a, b, preferred_element_type=F32)


def parts3(x):
    hi = jnp.clip(x, -BF16_MAX, BF16_MAX).astype(BF16)
    rest = x - hi.astype(F32)
    mid = rest.astype(BF16)
    low = (rest - mid.astype(F32)).astype(BF16)
    return hi, mid, low


def fetches(pairs, sems):
    return [pltpu.make_async_copy(src, dst, sems.at[i]) for i, (src, dst) in enumerate(pairs)]


def pack_kernel(keys_hbm, values_hbm, gates_hbm, out_ref, keys_ref, values_ref, gates_ref, sems):
    copies = fetches(
        [(gates_hbm, gates_ref), (keys_hbm, keys_ref), (values_hbm, values_ref)], sems
    )
    for copy in copies:
        copy.start()
    for copy in copies:
        copy.wait()
    hi, mid, low = parts3(gates_ref[...])
    ones = jnp.where(lax.broadcasted_iota(jnp.int32, (HEADS, TOK), 0) == 1, 1.0, 0.0)
    rows = [hi.astype(F32), mid.astype(F32), low.astype(F32), ones]
    out_ref[0:HEAD, :] = keys_ref[...]
    out_ref[HEAD : HEAD + 16, :] = jnp.concatenate(rows, axis=0).astype(BF16)
    out_ref[HEAD + 16 : BLOCK, :] = values_ref[...]


def pack(keys, values, gates):
    hbm = pl.BlockSpec(memory_space=pltpu.HBM)
    return pl.pallas_call(
        pack_kernel,
        out_shape=jax.ShapeDtypeStruct((BLOCK, TOK), BF16),
        in_specs=[hbm] * 3,
        out_specs=pl.BlockSpec(memory_space=pltpu.VMEM),
        scratch_shapes=[
            pltpu.VMEM((HEAD, TOK), BF16),
            pltpu.VMEM((HEAD, TOK), BF16),
            pltpu.VMEM((HEADS, TOK), F32),
            pltpu.SemaphoreType.DMA((3,)),
        ],
        compiler_params=PARAMS,
        name="pack",
    )(in_hbm(keys), in_hbm(values), in_hbm(gates))


def query_rows(query_ref):
    col = lax.broadcasted_iota(jnp.int32, (TOK, 16), 1)
    rows = []
    for h in range(HEADS):
        part = query_ref[:, h * HEAD : (h + 1) * HEAD] * jnp.asarray(0.125, BF16)
        takes = (col % HEADS == h) & (col < 3 * HEADS) | (col == 3 * HEADS)
        rows.append(jnp.concatenate([part, jnp.where(takes, -1.0, 0.0).astype(BF16)], axis=1))
    return jnp.concatenate(rows, axis=0)


def query_kernel(query_ref, out_ref):
    out_ref[...] = query_rows(query_ref)


def attend_kernel(count, place_ref, query_ref, source_ref, *refs):
    chunks, refs = refs[:count], refs[count:]
    out_ref, target_ref, m_ref, acc_ref, sem = refs
    copy = pltpu.make_async_copy(source_ref, target_ref, sem)
    copy.start()
    queries = query_ref[...]
    total_rows = HEADS * TOK
    row_of_gate = lax.broadcasted_iota(jnp.int32, (16, TOK), 0)

    def step(slot, fresh):
        key_rows = []
        for j, ref in enumerate(chunks):
            if fresh:
                bar = jnp.where(place_ref[1 + j] != 0, 0.0, -NEG).astype(BF16)
                gates = ref[slot, HEAD : HEAD + 16, :]
                gates = jnp.where(row_of_gate == 3 * HEADS, bar, gates)
                key_rows.append(jnp.concatenate([ref[slot, 0:HEAD, :], gates], axis=0))
            else:
                key_rows.append(ref[slot, 0 : HEAD + 16, :])
        value_rows = jnp.concatenate([ref[slot, HEAD:BLOCK, :] for ref in chunks], axis=1)
        scores = dot(queries, jnp.concatenate(key_rows, axis=1))
        if fresh:
            row = lax.broadcasted_iota(jnp.int32, (total_rows, TOK), 0) % TOK
            col = lax.broadcasted_iota(jnp.int32, (total_rows, TOK), 1)
            own = jnp.where(row >= col, scores[:, :TOK], NEG)
            scores = jnp.concatenate([own, scores[:, TOK:]], axis=1)
        peak = jnp.max(scores, axis=1, keepdims=True)
        if fresh:
            peak = jnp.broadcast_to(peak, (total_rows, TOK))
        else:
            before = m_ref[...]
            peak = jnp.maximum(before, peak)
        weights = jnp.exp(scores - jnp.concatenate([peak] * count, axis=1))
        product = lax.dot_general(
            weights.astype(BF16), value_rows, (((1,), (1,)), ((), ())), preferred_element_type=F32
        )
        m_ref[...] = peak
        if fresh:
            acc_ref[...] = product
        else:
            acc_ref[...] = acc_ref[...] * jnp.exp(before - peak)[:, : HEAD + 16] + product

    step(0, True)

    def body(slot, carry):
        step(slot, False)
        return carry

    lax.fori_loop(1, place_ref[0] + 1, body, 0)
    ones = 3 * HEADS + 1
    done = []
    for h in range(HEADS):
        here = slice(h * TOK, (h + 1) * TOK)
        done.append((acc_ref[here, 16:] / acc_ref[here, ones : ones + 1]).astype(BF16))
    out_ref[...] = jnp.concatenate(done, axis=1)
    copy.wait()


def attend(place, queries, weight, chunks):
    vmem = pl.BlockSpec(memory_space=pltpu.VMEM)
    total_rows = HEADS * TOK
    return pl.pallas_call(
        functools.partial(attend_kernel, len(chunks)),
        out_shape=[
            jax.ShapeDtypeStruct((TOK, HEADS * HEAD), BF16),
            jax.ShapeDtypeStruct(weight.shape, weight.dtype),
        ],
        in_specs=[pl.BlockSpec(memory_space=pltpu.SMEM), vmem]
        + [pl.BlockSpec(memory_space=pltpu.HBM)]
        + [vmem] * len(chunks),
        out_specs=[vmem] * 2,
        scratch_shapes=[
            pltpu.VMEM((total_rows, TOK), F32),
            pltpu.VMEM((total_rows, HEAD + 16), F32),
            pltpu.SemaphoreType.DMA,
        ],
        compiler_params=PARAMS,
        name="attend",
    )(place, in_vmem(queries), in_hbm(weight), *map(in_vmem, chunks))


def picks(routes_ref, transposed_slots=128):
    slot = lax.broadcasted_iota(jnp.int32, (transposed_slots, ROW), 0)
    expert, rank = slot // 2, slot % 2
    named0 = routes_ref[0:1, :] == expert
    named1 = routes_ref[1:2, :] == expert
    named = jnp.where(named0 | named1, 1.0, 0.0)
    earlier = lax.broadcasted_iota(jnp.int32, (ROW, ROW), 0) < lax.broadcasted_iota(
        jnp.int32, (ROW, ROW), 1
    )
    before = dot(named.astype(BF16), jnp.where(earlier, 1.0, 0.0).astype(BF16))
    chosen = before == rank.astype(F32)
    return chosen & named0, chosen & named1


def project_kernel(att_ref, weight_ref, residual_ref, gain_ref, routes_ref, stream_ref, rows_ref):
    total = residual_ref[...].astype(F32)
    both = jnp.concatenate([att_ref[x] for x in range(NT)], axis=1)
    total = total + dot(both, weight_ref[...])
    stream_ref[...] = total
    mean_square = jnp.mean(total * total, axis=1, keepdims=True)
    normed = (total * lax.rsqrt(mean_square + 1e-06) * gain_ref[...]).astype(BF16)
    first, second = picks(routes_ref)
    pick = jnp.where(first | second, 1.0, 0.0).astype(BF16)
    rows_ref[...] = dot(pick, normed).astype(BF16)


def hidden(rows, gate_ref, up_ref):
    gate = dot(rows, gate_ref[...])
    up = dot(rows, up_ref[...])
    return (gate / (1.0 + jnp.exp(-gate)) * up).astype(BF16)


def near_kernel(own, left0, right1, *refs):
    sources, outs, targets, sems = refs[:6], refs[6:9], refs[9:15], refs[15]
    copies = fetches(list(zip(sources, targets)), sems)
    for copy in copies:
        copy.start()
    copies[0].wait()
    copies[1].wait()
    for rows, out_ref in zip((own, left0, right1), outs):
        out_ref[...] = hidden(rows[...], targets[0], targets[1])
    for copy in copies[2:]:
        copy.wait()


def near(rows, weights):
    vmem = pl.BlockSpec(memory_space=pltpu.VMEM)
    wide = weights[0].shape[1]
    return pl.pallas_call(
        near_kernel,
        out_shape=[jax.ShapeDtypeStruct((r.shape[0], wide), BF16) for r in rows]
        + [jax.ShapeDtypeStruct(w.shape, w.dtype) for w in weights],
        in_specs=[vmem] * len(rows) + [pl.BlockSpec(memory_space=pltpu.HBM)] * len(weights),
        out_specs=[vmem] * (len(rows) + len(weights)),
        scratch_shapes=[pltpu.SemaphoreType.DMA((len(weights),))],
        compiler_params=PARAMS,
        name="near",
    )(*rows, *map(in_hbm, weights))


def rest_kernel(gate_ref, up_ref, left1, right0, h_left0, h_right1, h_left, h_right):
    half = TOK // 2
    h_left[:half, :] = h_left0[...]
    h_left[half:, :] = hidden(left1[...], gate_ref, up_ref)
    h_right[:half, :] = hidden(right0[...], gate_ref, up_ref)
    h_right[half:, :] = h_right1[...]


def far_kernel(gate_ref, up_ref, far0, far1, h_far):
    rows = jnp.concatenate([far0[...], far1[...]], axis=0)
    h_far[...] = hidden(rows, gate_ref, up_ref)


def down_kernel(own_ref, left_ref, right_ref, far_ref, w_own, w_left, w_right, w_far, out_ref):
    total = dot(own_ref[...], w_own[...])
    total = total + dot(left_ref[...], w_left[...])
    total = total + dot(right_ref[...], w_right[...])
    out_ref[...] = (total + dot(far_ref[...], w_far[...])).astype(BF16)


def combine_kernel(stream_ref, routes_ref, weight_ref, back_ref, out_ref):
    first, second = picks(routes_ref)
    spread = jnp.where(first, weight_ref[0:1, :], 0.0) + jnp.where(second, weight_ref[1:2, :], 0.0)
    back = back_ref[...]
    total = stream_ref[...]
    for part in parts3(spread):
        total = total + lax.dot_general(
            part, back, (((0,), (0,)), ((), ())), preferred_element_type=F32
        )
    out_ref[...] = total.astype(BF16)


def call(kernel, shapes, *args):
    return pl.pallas_call(
        kernel, out_shape=[jax.ShapeDtypeStruct(s, t) for s, t in shapes], compiler_params=PARAMS
    )(*args)


def moved(x, axis, by):
    size = {"z": NZ, "y": NY, "c": NC, "tp": NT}[axis]
    return lax.ppermute(x, axis, [(i, (i + by) % size) for i in range(size)])


def shards(
    queries,
    keys,
    values,
    forget_prefix_log,
    residual,
    out_weight,
    norm_gain,
    routes,
    route_weight,
    w_gate,
    w_up,
    w_down,
):
    z, y, c = lax.axis_index("z"), lax.axis_index("y"), lax.axis_index("c")
    down_own = w_down[0]
    down_left, down_right = moved(down_own, "tp", 1), moved(down_own, "tp", -1)
    block = pack(keys.T, values.T, forget_prefix_log.T)
    (rows_of_q,) = call(query_kernel, [((HEADS * TOK, HEAD + 16), BF16)], queries)
    fours = jnp.stack([block] + [moved(block, "z", step) for step in (2, 4, 6)])
    others = lax.ppermute(fours, "z", [(i, i ^ 1) for i in range(NZ)])
    own_order = y * NC + c
    chunks, kinds = [], []
    for name, group in (("first", fours), ("second", others)):
        for step in (0, 1, 3, 2):
            chunk = moved(group, "y", step) if step else group
            chunks += [chunk, moved(chunk, "c", 1)]
            for parity in (c, 1 - c):
                seen = (y - step) % NY * NC + parity <= own_order
                kinds.append(jnp.where(seen, 1, 0) if name == "first" else z % 2)
    place = jnp.stack([z // 2] + kinds).astype(jnp.int32)
    attended, out_w = attend(place, rows_of_q, out_weight, chunks)

    heads = lax.all_to_all(attended.reshape(NT, ROW, -1), "tp", 0, 0, tiled=True)
    far_source, _ = lax.optimization_barrier((down_own, heads))
    down_far = moved(far_source, "tp", 2)
    routes_row = routes.T
    stream, rows = call(
        project_kernel,
        [((ROW, D), F32), ((TOK, D), BF16)],
        heads,
        out_w,
        residual,
        norm_gain.reshape(1, D),
        routes_row,
    )
    arrived = lax.all_to_all(rows.reshape(64, 2, D), SP, 0, 0, tiled=True).reshape(TOK, D)
    half = TOK // 2
    top, bottom = arrived[:half], arrived[half:]
    left0, right1 = moved(top, "tp", 1), moved(bottom, "tp", -1)
    left1, right0 = moved(bottom, "tp", 1), moved(top, "tp", -1)
    far0, far1 = moved(left0, "tp", 1), moved(right1, "tp", -1)
    h_own, h_left0, h_right1, gate_w, up_w, *down_w = near(
        (arrived, left0, right1),
        (w_gate[0], w_up[0], down_own, down_left, down_right, down_far),
    )
    shape = (h_own.shape, BF16)
    h_left, h_right = call(rest_kernel, [shape] * 2, gate_w, up_w, left1, right0, h_left0, h_right1)
    from_left, from_right = moved(h_right, "tp", 1), moved(h_left, "tp", -1)
    (h_far,) = call(far_kernel, [shape], gate_w, up_w, far0, far1)
    (expert_out,) = call(
        down_kernel,
        [((TOK, D), BF16)],
        h_own,
        from_left,
        from_right,
        moved(h_far, "tp", 2),
        *down_w,
    )
    back = lax.all_to_all(expert_out.reshape(64, 2, D), SP, 0, 0, tiled=True).reshape(TOK, D)
    (out,) = call(
        combine_kernel, [((ROW, D), BF16)], stream, routes_row, route_weight.T, back
    )
    return out


def solution(mesh):
    split = Mesh(mesh.devices.reshape(NZ, NY, NC, NT), ("z", "y", "c", "tp"))
    rows = P(("z", "y", "c", "tp"), None)

    return jax.shard_map(
        shards,
        mesh=split,
        in_specs=(
            P(SP, "tp"),
            P(SP, "tp"),
            P(SP, "tp"),
            P(SP, "tp"),
            rows,
            P(),
            P(),
            rows,
            rows,
            P(SP, None, "tp"),
            P(SP, None, "tp"),
            P(SP, "tp", None),
        ),
        out_specs=rows,
        check_vma=False,
    )
```

```python
import functools

import jax
import jax.numpy as jnp
from jax import lax
from jax.experimental import pallas as pl
from jax.experimental.pallas import tpu as pltpu
from jax.sharding import Mesh, PartitionSpec as P


NZ, NY, NC, NT = 8, 4, 2, 4
TOK = 128
HEAD = 64
HEADS = 4
ROW = 32
D = 2048
BLOCK = TOK + 16
BF16_MAX = 3.3895313892515355e38
NEG = -3.0e38
F32 = jnp.float32
BF16 = jnp.bfloat16
SP = ("z", "y", "c")
PARAMS = pltpu.CompilerParams(vmem_limit_bytes=24 * 1024 * 1024)


def in_hbm(x):
    return pltpu.with_memory_space_constraint(x, pltpu.HBM)


def in_vmem(x):
    return pltpu.with_memory_space_constraint(x, pltpu.VMEM)


def dot(a, b):
    return jnp.dot(a, b, preferred_element_type=F32)


def parts3(x):
    hi = jnp.clip(x, -BF16_MAX, BF16_MAX).astype(BF16)
    rest = x - hi.astype(F32)
    mid = rest.astype(BF16)
    low = (rest - mid.astype(F32)).astype(BF16)
    return hi, mid, low


def fetches(pairs, sems):
    return [pltpu.make_async_copy(src, dst, sems.at[i]) for i, (src, dst) in enumerate(pairs)]


def pack_kernel(keys_hbm, values_hbm, gates_hbm, out_ref, keys_ref, values_ref, gates_ref, sems):
    copies = fetches(
        [(gates_hbm, gates_ref), (keys_hbm, keys_ref), (values_hbm, values_ref)], sems
    )
    for copy in copies:
        copy.start()
    for copy in copies:
        copy.wait()
    hi, mid, low = parts3(gates_ref[...])
    ones = jnp.where(lax.broadcasted_iota(jnp.int32, (HEADS, TOK), 0) == 1, 1.0, 0.0)
    rows = [hi.astype(F32), mid.astype(F32), low.astype(F32), ones]
    out_ref[0:HEAD, :] = keys_ref[...]
    out_ref[HEAD : HEAD + 16, :] = jnp.concatenate(rows, axis=0).astype(BF16)
    out_ref[HEAD + 16 : BLOCK, :] = values_ref[...]


def pack(keys, values, gates):
    hbm = pl.BlockSpec(memory_space=pltpu.HBM)
    return pl.pallas_call(
        pack_kernel,
        out_shape=jax.ShapeDtypeStruct((BLOCK, TOK), BF16),
        in_specs=[hbm] * 3,
        out_specs=pl.BlockSpec(memory_space=pltpu.VMEM),
        scratch_shapes=[
            pltpu.VMEM((HEAD, TOK), BF16),
            pltpu.VMEM((HEAD, TOK), BF16),
            pltpu.VMEM((HEADS, TOK), F32),
            pltpu.SemaphoreType.DMA((3,)),
        ],
        compiler_params=PARAMS,
        name="pack",
    )(in_hbm(keys), in_hbm(values), in_hbm(gates))


def query_rows(query_ref):
    col = lax.broadcasted_iota(jnp.int32, (TOK, 16), 1)
    rows = []
    for h in range(HEADS):
        part = query_ref[:, h * HEAD : (h + 1) * HEAD] * jnp.asarray(0.125, BF16)
        takes = (col % HEADS == h) & (col < 3 * HEADS) | (col == 3 * HEADS)
        rows.append(jnp.concatenate([part, jnp.where(takes, -1.0, 0.0).astype(BF16)], axis=1))
    return jnp.concatenate(rows, axis=0)


def query_kernel(query_ref, out_ref):
    out_ref[...] = query_rows(query_ref)


def attend_kernel(count, place_ref, query_ref, source_ref, *refs):
    chunks, refs = refs[:count], refs[count:]
    out_ref, target_ref, m_ref, acc_ref, sem = refs
    copy = pltpu.make_async_copy(source_ref, target_ref, sem)
    copy.start()
    queries = query_ref[...]
    total_rows = HEADS * TOK
    row_of_gate = lax.broadcasted_iota(jnp.int32, (16, TOK), 0)

    def step(slot, fresh):
        key_rows = []
        for j, ref in enumerate(chunks):
            if fresh:
                bar = jnp.where(place_ref[1 + j] != 0, 0.0, -NEG).astype(BF16)
                gates = ref[slot, HEAD : HEAD + 16, :]
                gates = jnp.where(row_of_gate == 3 * HEADS, bar, gates)
                key_rows.append(jnp.concatenate([ref[slot, 0:HEAD, :], gates], axis=0))
            else:
                key_rows.append(ref[slot, 0 : HEAD + 16, :])
        value_rows = jnp.concatenate([ref[slot, HEAD:BLOCK, :] for ref in chunks], axis=1)
        scores = dot(queries, jnp.concatenate(key_rows, axis=1))
        if fresh:
            row = lax.broadcasted_iota(jnp.int32, (total_rows, TOK), 0) % TOK
            col = lax.broadcasted_iota(jnp.int32, (total_rows, TOK), 1)
            own = jnp.where(row >= col, scores[:, :TOK], NEG)
            scores = jnp.concatenate([own, scores[:, TOK:]], axis=1)
        peak = jnp.max(scores, axis=1, keepdims=True)
        if fresh:
            peak = jnp.broadcast_to(peak, (total_rows, TOK))
        else:
            before = m_ref[...]
            peak = jnp.maximum(before, peak)
        weights = jnp.exp(scores - jnp.concatenate([peak] * count, axis=1))
        product = lax.dot_general(
            weights.astype(BF16), value_rows, (((1,), (1,)), ((), ())), preferred_element_type=F32
        )
        m_ref[...] = peak
        if fresh:
            acc_ref[...] = product
        else:
            acc_ref[...] = acc_ref[...] * jnp.exp(before - peak)[:, : HEAD + 16] + product

    step(0, True)

    def body(slot, carry):
        step(slot, False)
        return carry

    lax.fori_loop(1, place_ref[0] + 1, body, 0)
    ones = 3 * HEADS + 1
    done = []
    for h in range(HEADS):
        here = slice(h * TOK, (h + 1) * TOK)
        done.append((acc_ref[here, 16:] / acc_ref[here, ones : ones + 1]).astype(BF16))
    out_ref[...] = jnp.concatenate(done, axis=1)
    copy.wait()


def attend(place, queries, weight, chunks):
    vmem = pl.BlockSpec(memory_space=pltpu.VMEM)
    total_rows = HEADS * TOK
    return pl.pallas_call(
        functools.partial(attend_kernel, len(chunks)),
        out_shape=[
            jax.ShapeDtypeStruct((TOK, HEADS * HEAD), BF16),
            jax.ShapeDtypeStruct(weight.shape, weight.dtype),
        ],
        in_specs=[pl.BlockSpec(memory_space=pltpu.SMEM), vmem]
        + [pl.BlockSpec(memory_space=pltpu.HBM)]
        + [vmem] * len(chunks),
        out_specs=[vmem] * 2,
        scratch_shapes=[
            pltpu.VMEM((total_rows, TOK), F32),
            pltpu.VMEM((total_rows, HEAD + 16), F32),
            pltpu.SemaphoreType.DMA,
        ],
        compiler_params=PARAMS,
        name="attend",
    )(place, in_vmem(queries), in_hbm(weight), *map(in_vmem, chunks))


def picks(routes_ref, transposed_slots=128):
    slot = lax.broadcasted_iota(jnp.int32, (transposed_slots, ROW), 0)
    expert, rank = slot // 2, slot % 2
    named0 = routes_ref[0:1, :] == expert
    named1 = routes_ref[1:2, :] == expert
    named = jnp.where(named0 | named1, 1.0, 0.0)
    earlier = lax.broadcasted_iota(jnp.int32, (ROW, ROW), 0) < lax.broadcasted_iota(
        jnp.int32, (ROW, ROW), 1
    )
    before = dot(named.astype(BF16), jnp.where(earlier, 1.0, 0.0).astype(BF16))
    chosen = before == rank.astype(F32)
    return chosen & named0, chosen & named1


def project_kernel(att_ref, weight_ref, residual_ref, gain_ref, routes_ref, stream_ref, rows_ref):
    total = residual_ref[...].astype(F32)
    both = jnp.concatenate([att_ref[x] for x in range(NT)], axis=1)
    total = total + dot(both, weight_ref[...])
    stream_ref[...] = total
    mean_square = jnp.mean(total * total, axis=1, keepdims=True)
    normed = (total * lax.rsqrt(mean_square + 1e-06) * gain_ref[...]).astype(BF16)
    first, second = picks(routes_ref)
    pick = jnp.where(first | second, 1.0, 0.0).astype(BF16)
    rows_ref[...] = dot(pick, normed).astype(BF16).reshape(rows_ref.shape)


def hidden(rows, gate_ref, up_ref):
    rows = rows.reshape(-1, D)
    gate = dot(rows, gate_ref[...])
    up = dot(rows, up_ref[...])
    return (gate / (1.0 + jnp.exp(-gate)) * up).astype(BF16)


def near_kernel(own, left0, right1, *refs):
    sources, outs, targets, sems = refs[:5], refs[5:8], refs[8:13], refs[13]
    copies = fetches(list(zip(sources, targets)), sems)
    for copy in copies:
        copy.start()
    copies[0].wait()
    copies[1].wait()
    for rows, out_ref in zip((own, left0, right1), outs):
        out_ref[...] = hidden(rows[...], targets[0], targets[1])
    for copy in copies[2:]:
        copy.wait()


def near(rows, weights):
    vmem = pl.BlockSpec(memory_space=pltpu.VMEM)
    wide = weights[0].shape[1]
    return pl.pallas_call(
        near_kernel,
        out_shape=[jax.ShapeDtypeStruct((2 * r.shape[0], wide), BF16) for r in rows]
        + [jax.ShapeDtypeStruct(w.shape, w.dtype) for w in weights],
        in_specs=[vmem] * len(rows) + [pl.BlockSpec(memory_space=pltpu.HBM)] * len(weights),
        out_specs=[vmem] * (len(rows) + len(weights)),
        scratch_shapes=[pltpu.SemaphoreType.DMA((len(weights),))],
        compiler_params=PARAMS,
        name="near",
    )(*rows, *map(in_hbm, weights))


def rest_kernel(gate_ref, up_ref, left1, right0, h_left0, h_right1, h_left, h_right):
    half = TOK // 2
    h_left[:half, :] = h_left0[...]
    h_left[half:, :] = hidden(left1[...], gate_ref, up_ref)
    h_right[:half, :] = hidden(right0[...], gate_ref, up_ref)
    h_right[half:, :] = h_right1[...]


def far_kernel(gate_ref, up_ref, far0, far1, h_far):
    rows = jnp.concatenate([far0[...], far1[...]], axis=0)
    h_far[...] = hidden(rows, gate_ref, up_ref)


def down_kernel(own_ref, left_ref, right_ref, far_ref, w_own, w_left, w_right, w_far, out_ref):
    total = dot(own_ref[...], w_own[...])
    total = total + dot(left_ref[...], w_left[...])
    total = total + dot(right_ref[...], w_right[...])
    total = total + dot(far_ref[...], w_far[...])
    out_ref[...] = total.astype(BF16).reshape(out_ref.shape)


def combine_kernel(stream_ref, routes_ref, weight_ref, back_ref, out_ref):
    first, second = picks(routes_ref)
    spread = jnp.where(first, weight_ref[0:1, :], 0.0) + jnp.where(second, weight_ref[1:2, :], 0.0)
    back = back_ref[...].reshape(TOK, D)
    total = stream_ref[...]
    for part in parts3(spread):
        total = total + lax.dot_general(
            part, back, (((0,), (0,)), ((), ())), preferred_element_type=F32
        )
    out_ref[...] = total.astype(BF16)


def call(kernel, shapes, *args):
    return pl.pallas_call(
        kernel, out_shape=[jax.ShapeDtypeStruct(s, t) for s, t in shapes], compiler_params=PARAMS
    )(*args)


def moved(x, axis, by):
    size = {"z": NZ, "y": NY, "c": NC, "tp": NT}[axis]
    return lax.ppermute(x, axis, [(i, (i + by) % size) for i in range(size)])


def shards(
    queries,
    keys,
    values,
    forget_prefix_log,
    residual,
    out_weight,
    norm_gain,
    routes,
    route_weight,
    w_gate,
    w_up,
    w_down,
):
    z, y, c = lax.axis_index("z"), lax.axis_index("y"), lax.axis_index("c")
    down_own = w_down[0]
    down_left, down_right = moved(down_own, "tp", 1), moved(down_own, "tp", -1)
    block = pack(keys.T, values.T, forget_prefix_log.T)
    (rows_of_q,) = call(query_kernel, [((HEADS * TOK, HEAD + 16), BF16)], queries)
    fours = jnp.stack([block] + [moved(block, "z", step) for step in (2, 4, 6)])
    others = lax.ppermute(fours, "z", [(i, i ^ 1) for i in range(NZ)])
    own_order = y * NC + c
    chunks, kinds = [], []
    for name, group in (("first", fours), ("second", others)):
        for step in (0, 1, 3, 2):
            chunk = moved(group, "y", step) if step else group
            chunks += [chunk, moved(chunk, "c", 1)]
            for parity in (c, 1 - c):
                seen = (y - step) % NY * NC + parity <= own_order
                kinds.append(jnp.where(seen, 1, 0) if name == "first" else z % 2)
    place = jnp.stack([z // 2] + kinds).astype(jnp.int32)
    attended, out_w = attend(place, rows_of_q, out_weight, chunks)

    heads = lax.all_to_all(attended.reshape(NT, ROW, -1), "tp", 0, 0, tiled=True)
    far_source, _ = lax.optimization_barrier((down_own, heads))
    down_far = moved(far_source, "tp", 2)
    routes_row = routes.T
    stream, rows = call(
        project_kernel,
        [((ROW, D), F32), ((TOK // 2, 2, D), BF16)],
        heads,
        out_w,
        residual,
        norm_gain.reshape(1, D),
        routes_row,
    )
    arrived = lax.all_to_all(rows, SP, 0, 0, tiled=True)
    half = arrived.shape[0] // 2
    top, bottom = arrived[:half], arrived[half:]
    left0, right1 = moved(top, "tp", 1), moved(bottom, "tp", -1)
    left1, right0 = moved(bottom, "tp", 1), moved(top, "tp", -1)
    far0, far1 = moved(left0, "tp", 1), moved(right1, "tp", -1)
    h_own, h_left0, h_right1, gate_w, up_w, *down_w = near(
        (arrived, left0, right1),
        (w_gate[0], w_up[0], down_own, down_left, down_right),
    )
    shape = (h_own.shape, BF16)
    h_left, h_right = call(rest_kernel, [shape] * 2, gate_w, up_w, left1, right0, h_left0, h_right1)
    from_left, from_right = moved(h_right, "tp", 1), moved(h_left, "tp", -1)
    (h_far,) = call(far_kernel, [shape], gate_w, up_w, far0, far1)
    (expert_out,) = call(
        down_kernel,
        [((TOK // 2, 2, D), BF16)],
        h_own,
        from_left,
        from_right,
        moved(h_far, "tp", 2),
        *down_w,
        down_far,
    )
    back = lax.all_to_all(expert_out, SP, 0, 0, tiled=True)
    (out,) = call(
        combine_kernel, [((ROW, D), BF16)], stream, routes_row, route_weight.T, back
    )
    return out


def solution(mesh):
    split = Mesh(mesh.devices.reshape(NZ, NY, NC, NT), ("z", "y", "c", "tp"))
    rows = P(("z", "y", "c", "tp"), None)

    return jax.shard_map(
        shards,
        mesh=split,
        in_specs=(
            P(SP, "tp"),
            P(SP, "tp"),
            P(SP, "tp"),
            P(SP, "tp"),
            rows,
            P(),
            P(),
            rows,
            rows,
            P(SP, None, "tp"),
            P(SP, None, "tp"),
            P(SP, "tp", None),
        ),
        out_specs=rows,
        check_vma=False,
    )
```

```python
import functools

import jax
import jax.numpy as jnp
from jax import lax
from jax.experimental import pallas as pl
from jax.experimental.pallas import tpu as pltpu
from jax.sharding import Mesh, PartitionSpec as P


NZ, NY, NC, NT = 8, 4, 2, 4
TOK = 128
HEAD = 64
HEADS = 4
ROW = 32
D = 2048
BLOCK = TOK + 16
BF16_MAX = 3.3895313892515355e38
NEG = -3.0e38
F32 = jnp.float32
BF16 = jnp.bfloat16
SP = ("z", "y", "c")
PARAMS = pltpu.CompilerParams(vmem_limit_bytes=24 * 1024 * 1024)


def in_hbm(x):
    return pltpu.with_memory_space_constraint(x, pltpu.HBM)


def in_vmem(x):
    return pltpu.with_memory_space_constraint(x, pltpu.VMEM)


def dot(a, b):
    return jnp.dot(a, b, preferred_element_type=F32)


def parts3(x):
    hi = jnp.clip(x, -BF16_MAX, BF16_MAX).astype(BF16)
    rest = x - hi.astype(F32)
    mid = rest.astype(BF16)
    low = (rest - mid.astype(F32)).astype(BF16)
    return hi, mid, low


def fetches(pairs, sems):
    return [pltpu.make_async_copy(src, dst, sems.at[i]) for i, (src, dst) in enumerate(pairs)]


def pack_kernel(keys_hbm, values_hbm, gates_hbm, out_ref, keys_ref, values_ref, gates_ref, sems):
    copies = fetches(
        [(gates_hbm, gates_ref), (keys_hbm, keys_ref), (values_hbm, values_ref)], sems
    )
    for copy in copies:
        copy.start()
    for copy in copies:
        copy.wait()
    hi, mid, low = parts3(gates_ref[...])
    ones = jnp.where(lax.broadcasted_iota(jnp.int32, (HEADS, TOK), 0) == 1, 1.0, 0.0)
    rows = [hi.astype(F32), mid.astype(F32), low.astype(F32), ones]
    out_ref[0:HEAD, :] = keys_ref[...]
    out_ref[HEAD : HEAD + 16, :] = jnp.concatenate(rows, axis=0).astype(BF16)
    out_ref[HEAD + 16 : BLOCK, :] = values_ref[...]


def pack(keys, values, gates):
    hbm = pl.BlockSpec(memory_space=pltpu.HBM)
    return pl.pallas_call(
        pack_kernel,
        out_shape=jax.ShapeDtypeStruct((BLOCK, TOK), BF16),
        in_specs=[hbm] * 3,
        out_specs=pl.BlockSpec(memory_space=pltpu.VMEM),
        scratch_shapes=[
            pltpu.VMEM((HEAD, TOK), BF16),
            pltpu.VMEM((HEAD, TOK), BF16),
            pltpu.VMEM((HEADS, TOK), F32),
            pltpu.SemaphoreType.DMA((3,)),
        ],
        compiler_params=PARAMS,
        name="pack",
    )(in_hbm(keys), in_hbm(values), in_hbm(gates))


def query_rows(query_ref):
    col = lax.broadcasted_iota(jnp.int32, (TOK, 16), 1)
    rows = []
    for h in range(HEADS):
        part = query_ref[:, h * HEAD : (h + 1) * HEAD] * jnp.asarray(0.125, BF16)
        takes = (col % HEADS == h) & (col < 3 * HEADS) | (col == 3 * HEADS)
        rows.append(jnp.concatenate([part, jnp.where(takes, -1.0, 0.0).astype(BF16)], axis=1))
    return jnp.concatenate(rows, axis=0)


def query_kernel(query_ref, out_ref):
    out_ref[...] = query_rows(query_ref)


def attend_kernel(count, place_ref, query_ref, source_ref, *refs):
    chunks, refs = refs[:count], refs[count:]
    out_ref, target_ref, m_ref, acc_ref, sem = refs
    copy = pltpu.make_async_copy(source_ref, target_ref, sem)
    copy.start()
    queries = query_ref[...]
    total_rows = HEADS * TOK
    row_of_gate = lax.broadcasted_iota(jnp.int32, (16, TOK), 0)

    def step(slot, fresh):
        key_rows = []
        for j, ref in enumerate(chunks):
            if fresh:
                bar = jnp.where(place_ref[1 + j] != 0, 0.0, -NEG).astype(BF16)
                gates = ref[slot, HEAD : HEAD + 16, :]
                gates = jnp.where(row_of_gate == 3 * HEADS, bar, gates)
                key_rows.append(jnp.concatenate([ref[slot, 0:HEAD, :], gates], axis=0))
            else:
                key_rows.append(ref[slot, 0 : HEAD + 16, :])
        value_rows = jnp.concatenate([ref[slot, HEAD:BLOCK, :] for ref in chunks], axis=1)
        scores = dot(queries, jnp.concatenate(key_rows, axis=1))
        if fresh:
            row = lax.broadcasted_iota(jnp.int32, (total_rows, TOK), 0) % TOK
            col = lax.broadcasted_iota(jnp.int32, (total_rows, TOK), 1)
            own = jnp.where(row >= col, scores[:, :TOK], NEG)
            scores = jnp.concatenate([own, scores[:, TOK:]], axis=1)
        peak = jnp.max(scores, axis=1, keepdims=True)
        if fresh:
            peak = jnp.broadcast_to(peak, (total_rows, TOK))
        else:
            before = m_ref[...]
            peak = jnp.maximum(before, peak)
        weights = jnp.exp(scores - jnp.concatenate([peak] * count, axis=1))
        product = lax.dot_general(
            weights.astype(BF16), value_rows, (((1,), (1,)), ((), ())), preferred_element_type=F32
        )
        m_ref[...] = peak
        if fresh:
            acc_ref[...] = product
        else:
            acc_ref[...] = acc_ref[...] * jnp.exp(before - peak)[:, : HEAD + 16] + product

    step(0, True)

    def body(slot, carry):
        step(slot, False)
        return carry

    lax.fori_loop(1, place_ref[0] + 1, body, 0)
    ones = 3 * HEADS + 1
    done = []
    for h in range(HEADS):
        here = slice(h * TOK, (h + 1) * TOK)
        done.append((acc_ref[here, 16:] / acc_ref[here, ones : ones + 1]).astype(BF16))
    out_ref[...] = jnp.concatenate(done, axis=1)
    copy.wait()


def attend(place, queries, weight, chunks):
    vmem = pl.BlockSpec(memory_space=pltpu.VMEM)
    total_rows = HEADS * TOK
    return pl.pallas_call(
        functools.partial(attend_kernel, len(chunks)),
        out_shape=[
            jax.ShapeDtypeStruct((TOK, HEADS * HEAD), BF16),
            jax.ShapeDtypeStruct(weight.shape, weight.dtype),
        ],
        in_specs=[pl.BlockSpec(memory_space=pltpu.SMEM), vmem]
        + [pl.BlockSpec(memory_space=pltpu.HBM)]
        + [vmem] * len(chunks),
        out_specs=[vmem] * 2,
        scratch_shapes=[
            pltpu.VMEM((total_rows, TOK), F32),
            pltpu.VMEM((total_rows, HEAD + 16), F32),
            pltpu.SemaphoreType.DMA,
        ],
        compiler_params=PARAMS,
        name="attend",
    )(place, in_vmem(queries), in_hbm(weight), *map(in_vmem, chunks))


def picks(routes_ref, transposed_slots=128):
    slot = lax.broadcasted_iota(jnp.int32, (transposed_slots, ROW), 0)
    expert, rank = slot // 2, slot % 2
    named0 = routes_ref[0:1, :] == expert
    named1 = routes_ref[1:2, :] == expert
    named = jnp.where(named0 | named1, 1.0, 0.0)
    earlier = lax.broadcasted_iota(jnp.int32, (ROW, ROW), 0) < lax.broadcasted_iota(
        jnp.int32, (ROW, ROW), 1
    )
    before = dot(named.astype(BF16), jnp.where(earlier, 1.0, 0.0).astype(BF16))
    chosen = before == rank.astype(F32)
    return chosen & named0, chosen & named1


def project_kernel(att_ref, weight_ref, residual_ref, gain_ref, routes_ref, stream_ref, rows_ref):
    total = residual_ref[...].astype(F32)
    both = jnp.concatenate([att_ref[x] for x in range(NT)], axis=1)
    total = total + dot(both, weight_ref[...])
    stream_ref[...] = total
    mean_square = jnp.mean(total * total, axis=1, keepdims=True)
    normed = (total * lax.rsqrt(mean_square + 1e-06) * gain_ref[...]).astype(BF16)
    first, second = picks(routes_ref)
    pick = jnp.where(first | second, 1.0, 0.0).astype(BF16)
    rows_ref[...] = dot(pick, normed).astype(BF16).reshape(rows_ref.shape)


def hidden(rows, gate_ref, up_ref):
    rows = rows.reshape(-1, D)
    gate = dot(rows, gate_ref[...])
    up = dot(rows, up_ref[...])
    return (gate / (1.0 + jnp.exp(-gate)) * up).astype(BF16)


def near_kernel(own, left0, right1, *refs):
    sources, outs, targets, sems = refs[:5], refs[5:8], refs[8:13], refs[13]
    copies = fetches(list(zip(sources, targets)), sems)
    for copy in copies:
        copy.start()
    copies[0].wait()
    copies[1].wait()
    for rows, out_ref in zip((own, left0, right1), outs):
        out_ref[...] = hidden(rows[...], targets[0], targets[1])
    for copy in copies[2:]:
        copy.wait()


def near(rows, weights):
    vmem = pl.BlockSpec(memory_space=pltpu.VMEM)
    wide = weights[0].shape[1]
    return pl.pallas_call(
        near_kernel,
        out_shape=[jax.ShapeDtypeStruct((2 * r.shape[0], wide), BF16) for r in rows]
        + [jax.ShapeDtypeStruct(w.shape, w.dtype) for w in weights],
        in_specs=[vmem] * len(rows) + [pl.BlockSpec(memory_space=pltpu.HBM)] * len(weights),
        out_specs=[vmem] * (len(rows) + len(weights)),
        scratch_shapes=[pltpu.SemaphoreType.DMA((len(weights),))],
        compiler_params=PARAMS,
        name="near",
    )(*rows, *map(in_hbm, weights))


def rest_kernel(gate_ref, up_ref, left1, right0, h_left0, h_right1, h_left, h_right):
    half = TOK // 2
    h_left[:half, :] = h_left0[...]
    h_left[half:, :] = hidden(left1[...], gate_ref, up_ref)
    h_right[:half, :] = hidden(right0[...], gate_ref, up_ref)
    h_right[half:, :] = h_right1[...]


def far_kernel(gate_ref, up_ref, far0, far1, h_far):
    rows = jnp.concatenate([far0[...], far1[...]], axis=0)
    h_far[...] = hidden(rows, gate_ref, up_ref)


def part_kernel(own_ref, left_ref, right_ref, w_own, w_left, w_right, out_ref):
    total = dot(own_ref[...], w_own[...])
    total = total + dot(left_ref[...], w_left[...])
    out_ref[...] = total + dot(right_ref[...], w_right[...])


def down_kernel(part_ref, far_ref, w_far, out_ref):
    total = part_ref[...] + dot(far_ref[...], w_far[...])
    out_ref[...] = total.astype(BF16).reshape(out_ref.shape)


def combine_kernel(stream_ref, routes_ref, weight_ref, back_ref, out_ref):
    first, second = picks(routes_ref)
    spread = jnp.where(first, weight_ref[0:1, :], 0.0) + jnp.where(second, weight_ref[1:2, :], 0.0)
    back = back_ref[...].reshape(TOK, D)
    total = stream_ref[...]
    for part in parts3(spread):
        total = total + lax.dot_general(
            part, back, (((0,), (0,)), ((), ())), preferred_element_type=F32
        )
    out_ref[...] = total.astype(BF16)


def call(kernel, shapes, *args):
    return pl.pallas_call(
        kernel, out_shape=[jax.ShapeDtypeStruct(s, t) for s, t in shapes], compiler_params=PARAMS
    )(*args)


def moved(x, axis, by):
    size = {"z": NZ, "y": NY, "c": NC, "tp": NT}[axis]
    return lax.ppermute(x, axis, [(i, (i + by) % size) for i in range(size)])


def shards(
    queries,
    keys,
    values,
    forget_prefix_log,
    residual,
    out_weight,
    norm_gain,
    routes,
    route_weight,
    w_gate,
    w_up,
    w_down,
):
    z, y, c = lax.axis_index("z"), lax.axis_index("y"), lax.axis_index("c")
    down_own = w_down[0]
    down_left, down_right = moved(down_own, "tp", 1), moved(down_own, "tp", -1)
    block = pack(keys.T, values.T, forget_prefix_log.T)
    (rows_of_q,) = call(query_kernel, [((HEADS * TOK, HEAD + 16), BF16)], queries)
    fours = jnp.stack([block] + [moved(block, "z", step) for step in (2, 4, 6)])
    others = lax.ppermute(fours, "z", [(i, i ^ 1) for i in range(NZ)])
    own_order = y * NC + c
    chunks, kinds = [], []
    for name, group in (("first", fours), ("second", others)):
        for step in (0, 1, 3, 2):
            chunk = moved(group, "y", step) if step else group
            chunks += [chunk, moved(chunk, "c", 1)]
            for parity in (c, 1 - c):
                seen = (y - step) % NY * NC + parity <= own_order
                kinds.append(jnp.where(seen, 1, 0) if name == "first" else z % 2)
    place = jnp.stack([z // 2] + kinds).astype(jnp.int32)
    attended, out_w = attend(place, rows_of_q, out_weight, chunks)

    heads = lax.all_to_all(attended.reshape(NT, ROW, -1), "tp", 0, 0, tiled=True)
    far_source, _ = lax.optimization_barrier((down_own, heads))
    down_far = moved(far_source, "tp", 2)
    routes_row = routes.T
    stream, rows = call(
        project_kernel,
        [((ROW, D), F32), ((TOK // 2, 2, D), BF16)],
        heads,
        out_w,
        residual,
        norm_gain.reshape(1, D),
        routes_row,
    )
    arrived = lax.all_to_all(rows, SP, 0, 0, tiled=True)
    half = arrived.shape[0] // 2
    top, bottom = arrived[:half], arrived[half:]
    left0, right1 = moved(top, "tp", 1), moved(bottom, "tp", -1)
    left1, right0 = moved(bottom, "tp", 1), moved(top, "tp", -1)
    far0, far1 = moved(left0, "tp", 1), moved(right1, "tp", -1)
    h_own, h_left0, h_right1, gate_w, up_w, *down_w = near(
        (arrived, left0, right1),
        (w_gate[0], w_up[0], down_own, down_left, down_right),
    )
    shape = (h_own.shape, BF16)
    h_left, h_right = call(rest_kernel, [shape] * 2, gate_w, up_w, left1, right0, h_left0, h_right1)
    from_left, from_right = moved(h_right, "tp", 1), moved(h_left, "tp", -1)
    (h_far,) = call(far_kernel, [shape], gate_w, up_w, far0, far1)
    from_far = moved(h_far, "tp", 2)
    (part,) = call(
        part_kernel, [((TOK, D), F32)], h_own, from_left, from_right, *down_w
    )
    (expert_out,) = call(
        down_kernel, [((TOK // 2, 2, D), BF16)], in_vmem(part), from_far, down_far
    )
    back = lax.all_to_all(expert_out, SP, 0, 0, tiled=True)
    (out,) = call(
        combine_kernel, [((ROW, D), BF16)], stream, routes_row, route_weight.T, back
    )
    return out


def solution(mesh):
    split = Mesh(mesh.devices.reshape(NZ, NY, NC, NT), ("z", "y", "c", "tp"))
    rows = P(("z", "y", "c", "tp"), None)

    return jax.shard_map(
        shards,
        mesh=split,
        in_specs=(
            P(SP, "tp"),
            P(SP, "tp"),
            P(SP, "tp"),
            P(SP, "tp"),
            rows,
            P(),
            P(),
            rows,
            rows,
            P(SP, None, "tp"),
            P(SP, None, "tp"),
            P(SP, "tp", None),
        ),
        out_specs=rows,
        check_vma=False,
    )
```

```python
import functools

import jax
import jax.numpy as jnp
from jax import lax
from jax.experimental import pallas as pl
from jax.experimental.pallas import tpu as pltpu
from jax.sharding import Mesh, PartitionSpec as P


NZ, NY, NC, NT = 8, 4, 2, 4
TOK = 128
HEAD = 64
HEADS = 4
ROW = 32
TP_STEPS = (0, 2, 1, 3)
D = 2048
BLOCK = TOK + 16
BF16_MAX = 3.3895313892515355e38
NEG = -3.0e38
F32 = jnp.float32
BF16 = jnp.bfloat16
SP = ("z", "y", "c")
PARAMS = pltpu.CompilerParams(vmem_limit_bytes=24 * 1024 * 1024)


def in_hbm(x):
    return pltpu.with_memory_space_constraint(x, pltpu.HBM)


def in_vmem(x):
    return pltpu.with_memory_space_constraint(x, pltpu.VMEM)


def dot(a, b):
    return jnp.dot(a, b, preferred_element_type=F32)


def parts3(x):
    hi = jnp.clip(x, -BF16_MAX, BF16_MAX).astype(BF16)
    rest = x - hi.astype(F32)
    mid = rest.astype(BF16)
    low = (rest - mid.astype(F32)).astype(BF16)
    return hi, mid, low


def fetches(pairs, sems):
    return [pltpu.make_async_copy(src, dst, sems.at[i]) for i, (src, dst) in enumerate(pairs)]


def pack_kernel(keys_hbm, values_hbm, gates_hbm, out_ref, keys_ref, values_ref, gates_ref, sems):
    copies = fetches(
        [(gates_hbm, gates_ref), (keys_hbm, keys_ref), (values_hbm, values_ref)], sems
    )
    for copy in copies:
        copy.start()
    for copy in copies:
        copy.wait()
    hi, mid, low = parts3(gates_ref[...])
    ones = jnp.where(lax.broadcasted_iota(jnp.int32, (HEADS, TOK), 0) == 1, 1.0, 0.0)
    rows = [hi.astype(F32), mid.astype(F32), low.astype(F32), ones]
    out_ref[0:HEAD, :] = keys_ref[...]
    out_ref[HEAD : HEAD + 16, :] = jnp.concatenate(rows, axis=0).astype(BF16)
    out_ref[HEAD + 16 : BLOCK, :] = values_ref[...]


def pack(keys, values, gates):
    hbm = pl.BlockSpec(memory_space=pltpu.HBM)
    return pl.pallas_call(
        pack_kernel,
        out_shape=jax.ShapeDtypeStruct((BLOCK, TOK), BF16),
        in_specs=[hbm] * 3,
        out_specs=pl.BlockSpec(memory_space=pltpu.VMEM),
        scratch_shapes=[
            pltpu.VMEM((HEAD, TOK), BF16),
            pltpu.VMEM((HEAD, TOK), BF16),
            pltpu.VMEM((HEADS, TOK), F32),
            pltpu.SemaphoreType.DMA((3,)),
        ],
        compiler_params=PARAMS,
        name="pack",
    )(in_hbm(keys), in_hbm(values), in_hbm(gates))


def query_rows(query_ref):
    col = lax.broadcasted_iota(jnp.int32, (TOK, 16), 1)
    rows = []
    for h in range(HEADS):
        part = query_ref[:, h * HEAD : (h + 1) * HEAD] * jnp.asarray(0.125, BF16)
        takes = (col % HEADS == h) & (col < 3 * HEADS) | (col == 3 * HEADS)
        rows.append(jnp.concatenate([part, jnp.where(takes, -1.0, 0.0).astype(BF16)], axis=1))
    return jnp.concatenate(rows, axis=0)


def query_kernel(query_ref, out_ref):
    out_ref[...] = query_rows(query_ref)


def attend_kernel(count, place_ref, query_ref, source_ref, *refs):
    chunks, refs = refs[:count], refs[count:]
    outs, (target_ref, m_ref, acc_ref, done_ref, sem) = refs[:NT], refs[NT:]
    copy = pltpu.make_async_copy(source_ref, target_ref, sem)
    copy.start()
    queries = query_ref[...]
    total_rows = HEADS * TOK
    row_of_gate = lax.broadcasted_iota(jnp.int32, (16, TOK), 0)

    def step(slot, fresh):
        key_rows = []
        for j, ref in enumerate(chunks):
            if fresh:
                bar = jnp.where(place_ref[1 + j] != 0, 0.0, -NEG).astype(BF16)
                gates = ref[slot, HEAD : HEAD + 16, :]
                gates = jnp.where(row_of_gate == 3 * HEADS, bar, gates)
                key_rows.append(jnp.concatenate([ref[slot, 0:HEAD, :], gates], axis=0))
            else:
                key_rows.append(ref[slot, 0 : HEAD + 16, :])
        value_rows = jnp.concatenate([ref[slot, HEAD:BLOCK, :] for ref in chunks], axis=1)
        scores = dot(queries, jnp.concatenate(key_rows, axis=1))
        if fresh:
            row = lax.broadcasted_iota(jnp.int32, (total_rows, TOK), 0) % TOK
            col = lax.broadcasted_iota(jnp.int32, (total_rows, TOK), 1)
            own = jnp.where(row >= col, scores[:, :TOK], NEG)
            scores = jnp.concatenate([own, scores[:, TOK:]], axis=1)
        peak = jnp.max(scores, axis=1, keepdims=True)
        if fresh:
            peak = jnp.broadcast_to(peak, (total_rows, TOK))
        else:
            before = m_ref[...]
            peak = jnp.maximum(before, peak)
        weights = jnp.exp(scores - jnp.concatenate([peak] * count, axis=1))
        product = lax.dot_general(
            weights.astype(BF16), value_rows, (((1,), (1,)), ((), ())), preferred_element_type=F32
        )
        m_ref[...] = peak
        if fresh:
            acc_ref[...] = product
        else:
            acc_ref[...] = acc_ref[...] * jnp.exp(before - peak)[:, : HEAD + 16] + product

    step(0, True)

    def body(slot, carry):
        step(slot, False)
        return carry

    lax.fori_loop(1, place_ref[0] + 1, body, 0)
    ones = 3 * HEADS + 1
    done = []
    for h in range(HEADS):
        here = slice(h * TOK, (h + 1) * TOK)
        done.append((acc_ref[here, 16:] / acc_ref[here, ones : ones + 1]).astype(BF16))
    done_ref[...] = jnp.concatenate(done, axis=1)
    own_x = place_ref[1 + count]
    for step, out_ref in zip(TP_STEPS, outs):
        out_ref[...] = done_ref[pl.ds((own_x + step) % NT * ROW, ROW), :]
    copy.wait()


def attend(place, queries, weight, chunks):
    vmem = pl.BlockSpec(memory_space=pltpu.VMEM)
    total_rows = HEADS * TOK
    return pl.pallas_call(
        functools.partial(attend_kernel, len(chunks)),
        out_shape=[jax.ShapeDtypeStruct((ROW, HEADS * HEAD), BF16)] * NT
        + [jax.ShapeDtypeStruct(weight.shape, weight.dtype)],
        in_specs=[pl.BlockSpec(memory_space=pltpu.SMEM), vmem]
        + [pl.BlockSpec(memory_space=pltpu.HBM)]
        + [vmem] * len(chunks),
        out_specs=[vmem] * (NT + 1),
        scratch_shapes=[
            pltpu.VMEM((total_rows, TOK), F32),
            pltpu.VMEM((total_rows, HEAD + 16), F32),
            pltpu.VMEM((TOK, HEADS * HEAD), BF16),
            pltpu.SemaphoreType.DMA,
        ],
        compiler_params=PARAMS,
        name="attend",
    )(place, in_vmem(queries), in_hbm(weight), *map(in_vmem, chunks))


def picks(routes_ref, transposed_slots=128):
    slot = lax.broadcasted_iota(jnp.int32, (transposed_slots, ROW), 0)
    expert, rank = slot // 2, slot % 2
    named0 = routes_ref[0:1, :] == expert
    named1 = routes_ref[1:2, :] == expert
    named = jnp.where(named0 | named1, 1.0, 0.0)
    earlier = lax.broadcasted_iota(jnp.int32, (ROW, ROW), 0) < lax.broadcasted_iota(
        jnp.int32, (ROW, ROW), 1
    )
    before = dot(named.astype(BF16), jnp.where(earlier, 1.0, 0.0).astype(BF16))
    chosen = before == rank.astype(F32)
    return chosen & named0, chosen & named1


def project_kernel(
    place_ref, h0, h2, h1, h3, weight_ref, residual_ref, gain_ref, routes_ref, stream_ref, rows_ref
):
    total = residual_ref[...].astype(F32)
    wide = HEADS * HEAD
    for step, ref in zip(TP_STEPS, (h0, h2, h1, h3)):
        begin = (place_ref[0] + NT - step) % NT * wide
        total = total + dot(ref[...], weight_ref[pl.ds(begin, wide), :])
    stream_ref[...] = total
    mean_square = jnp.mean(total * total, axis=1, keepdims=True)
    normed = (total * lax.rsqrt(mean_square + 1e-06) * gain_ref[...]).astype(BF16)
    first, second = picks(routes_ref)
    pick = jnp.where(first | second, 1.0, 0.0).astype(BF16)
    rows_ref[...] = dot(pick, normed).astype(BF16).reshape(rows_ref.shape)


def project(*args):
    vmem = pl.BlockSpec(memory_space=pltpu.VMEM)
    return pl.pallas_call(
        project_kernel,
        out_shape=[
            jax.ShapeDtypeStruct((ROW, D), F32),
            jax.ShapeDtypeStruct((TOK // 2, 2, D), BF16),
        ],
        in_specs=[pl.BlockSpec(memory_space=pltpu.SMEM)] + [vmem] * (len(args) - 1),
        out_specs=[vmem] * 2,
        compiler_params=PARAMS,
        name="project",
    )(*args)


def hidden(rows, gate_ref, up_ref):
    rows = rows.reshape(-1, D)
    gate = dot(rows, gate_ref[...])
    up = dot(rows, up_ref[...])
    return (gate / (1.0 + jnp.exp(-gate)) * up).astype(BF16)


def near_kernel(own, left0, right1, *refs):
    sources, outs, targets, sems = refs[:5], refs[5:8], refs[8:13], refs[13]
    copies = fetches(list(zip(sources, targets)), sems)
    for copy in copies:
        copy.start()
    copies[0].wait()
    copies[1].wait()
    for rows, out_ref in zip((own, left0, right1), outs):
        out_ref[...] = hidden(rows[...], targets[0], targets[1])
    for copy in copies[2:]:
        copy.wait()


def near(rows, weights):
    vmem = pl.BlockSpec(memory_space=pltpu.VMEM)
    wide = weights[0].shape[1]
    return pl.pallas_call(
        near_kernel,
        out_shape=[jax.ShapeDtypeStruct((2 * r.shape[0], wide), BF16) for r in rows]
        + [jax.ShapeDtypeStruct(w.shape, w.dtype) for w in weights],
        in_specs=[vmem] * len(rows) + [pl.BlockSpec(memory_space=pltpu.HBM)] * len(weights),
        out_specs=[vmem] * (len(rows) + len(weights)),
        scratch_shapes=[pltpu.SemaphoreType.DMA((len(weights),))],
        compiler_params=PARAMS,
        name="near",
    )(*rows, *map(in_hbm, weights))


def rest_kernel(gate_ref, up_ref, left1, right0, h_left0, h_right1, h_left, h_right):
    half = TOK // 2
    h_left[:half, :] = h_left0[...]
    h_left[half:, :] = hidden(left1[...], gate_ref, up_ref)
    h_right[:half, :] = hidden(right0[...], gate_ref, up_ref)
    h_right[half:, :] = h_right1[...]


def far_kernel(gate_ref, up_ref, far0, far1, h_far):
    rows = jnp.concatenate([far0[...], far1[...]], axis=0)
    h_far[...] = hidden(rows, gate_ref, up_ref)


def part_kernel(own_ref, left_ref, right_ref, w_own, w_left, w_right, out_ref):
    total = dot(own_ref[...], w_own[...])
    total = total + dot(left_ref[...], w_left[...])
    out_ref[...] = total + dot(right_ref[...], w_right[...])


def down_kernel(part_ref, far_ref, w_far, out_ref):
    total = part_ref[...] + dot(far_ref[...], w_far[...])
    out_ref[...] = total.astype(BF16).reshape(out_ref.shape)


def combine_kernel(stream_ref, routes_ref, weight_ref, back_ref, out_ref):
    first, second = picks(routes_ref)
    spread = jnp.where(first, weight_ref[0:1, :], 0.0) + jnp.where(second, weight_ref[1:2, :], 0.0)
    back = back_ref[...].reshape(TOK, D)
    total = stream_ref[...]
    for part in parts3(spread):
        total = total + lax.dot_general(
            part, back, (((0,), (0,)), ((), ())), preferred_element_type=F32
        )
    out_ref[...] = total.astype(BF16)


def call(kernel, shapes, *args):
    return pl.pallas_call(
        kernel, out_shape=[jax.ShapeDtypeStruct(s, t) for s, t in shapes], compiler_params=PARAMS
    )(*args)


def moved(x, axis, by):
    size = {"z": NZ, "y": NY, "c": NC, "tp": NT}[axis]
    return lax.ppermute(x, axis, [(i, (i + by) % size) for i in range(size)])


def shards(
    queries,
    keys,
    values,
    forget_prefix_log,
    residual,
    out_weight,
    norm_gain,
    routes,
    route_weight,
    w_gate,
    w_up,
    w_down,
):
    z, y, c = lax.axis_index("z"), lax.axis_index("y"), lax.axis_index("c")
    down_own = w_down[0]
    down_left, down_right = moved(down_own, "tp", 1), moved(down_own, "tp", -1)
    block = pack(keys.T, values.T, forget_prefix_log.T)
    (rows_of_q,) = call(query_kernel, [((HEADS * TOK, HEAD + 16), BF16)], queries)
    fours = jnp.stack([block] + [moved(block, "z", step) for step in (2, 4, 6)])
    others = lax.ppermute(fours, "z", [(i, i ^ 1) for i in range(NZ)])
    own_order = y * NC + c
    chunks, kinds = [], []
    for name, group in (("first", fours), ("second", others)):
        for step in (0, 1, 3, 2):
            chunk = moved(group, "y", step) if step else group
            chunks += [chunk, moved(chunk, "c", 1)]
            for parity in (c, 1 - c):
                seen = (y - step) % NY * NC + parity <= own_order
                kinds.append(jnp.where(seen, 1, 0) if name == "first" else z % 2)
    x = lax.axis_index("tp")
    place = jnp.stack([z // 2] + kinds + [x]).astype(jnp.int32)
    *attended, out_w = attend(place, rows_of_q, out_weight, chunks)

    heads = [attended[0]] + [
        moved(part, "tp", step) for part, step in zip(attended[1:], TP_STEPS[1:])
    ]
    far_source = down_own
    down_far = moved(far_source, "tp", 2)
    routes_row = routes.T
    stream, rows = project(
        x.reshape(1).astype(jnp.int32),
        *heads,
        out_w,
        residual,
        norm_gain.reshape(1, D),
        routes_row,
    )
    arrived = lax.all_to_all(rows, SP, 0, 0, tiled=True)
    half = arrived.shape[0] // 2
    top, bottom = arrived[:half], arrived[half:]
    left0, right1 = moved(top, "tp", 1), moved(bottom, "tp", -1)
    left1, right0 = moved(bottom, "tp", 1), moved(top, "tp", -1)
    far0, far1 = moved(left0, "tp", 1), moved(right1, "tp", -1)
    h_own, h_left0, h_right1, gate_w, up_w, *down_w = near(
        (arrived, left0, right1),
        (w_gate[0], w_up[0], down_own, down_left, down_right),
    )
    shape = (h_own.shape, BF16)
    h_left, h_right = call(rest_kernel, [shape] * 2, gate_w, up_w, left1, right0, h_left0, h_right1)
    from_left, from_right = moved(h_right, "tp", 1), moved(h_left, "tp", -1)
    (h_far,) = call(far_kernel, [shape], gate_w, up_w, far0, far1)
    from_far = moved(h_far, "tp", 2)
    (part,) = call(
        part_kernel, [((TOK, D), F32)], h_own, from_left, from_right, *down_w
    )
    (expert_out,) = call(
        down_kernel, [((TOK // 2, 2, D), BF16)], in_vmem(part), from_far, down_far
    )
    back = lax.all_to_all(expert_out, SP, 0, 0, tiled=True)
    (out,) = call(
        combine_kernel, [((ROW, D), BF16)], stream, routes_row, route_weight.T, back
    )
    return out


def solution(mesh):
    split = Mesh(mesh.devices.reshape(NZ, NY, NC, NT), ("z", "y", "c", "tp"))
    rows = P(("z", "y", "c", "tp"), None)

    return jax.shard_map(
        shards,
        mesh=split,
        in_specs=(
            P(SP, "tp"),
            P(SP, "tp"),
            P(SP, "tp"),
            P(SP, "tp"),
            rows,
            P(),
            P(),
            rows,
            rows,
            P(SP, None, "tp"),
            P(SP, None, "tp"),
            P(SP, "tp", None),
        ),
        out_specs=rows,
        check_vma=False,
    )
```
